128 devices in a mesh: sp: 32 (over z, y, core), tp: 4 (over x).
Axes of the slice: x: 4, y: 4, z: 4, core: 2. Of those that a mesh axis runs over, the one named last changes fastest.
Arguments:
- residual_input_stream: bfloat16 [24576, 2048], P('sp'), may hold values from -6 to 6
- projected_queries: bfloat16 [24576, 512], P('sp', 'tp'), may hold values from -6 to 6
- projected_keys: bfloat16 [24576, 512], P('sp', 'tp'), may hold values from -6 to 6
- projected_values: bfloat16 [24576, 1024], P('sp', 'tp'), may hold values from -6 to 6
- emitted_switch_entries: bfloat16 [24576, 1024], P('sp', 'tp'), may hold values from -6 to 6
- retention_preactivations: bfloat16 [24576, 512], P('sp', 'tp'), may hold values from -6 to 15
- additional_fading_amount: float32 [24576], P('sp'), may hold values from -2 to 0
- head_norm_gain: float32 [128], replicated, may hold values from 0.1 to 1.9
- attention_output_weight: bfloat16 [1024, 2048], P('tp'), may hold values from -0.1875 to 0.1875
- feedforward_norm_gain: float32 [2048], replicated, may hold values from 0.1 to 1.9
- gate_up_matrix: bfloat16 [2048, 5632], P('sp', 'tp'), may hold values from -0.125 to 0.125
- value_up_matrix: bfloat16 [2048, 5632], P('sp', 'tp'), may hold values from -0.125 to 0.125
- gate_filter_taps: bfloat16 [3, 5632], P(None, 'tp'), may hold values from -3.5 to 3.5
- value_filter_taps: bfloat16 [3, 5632], P(None, 'tp'), may hold values from -3.5 to 3.5
- down_projection_weight: bfloat16 [5632, 2048], P('tp', 'sp'), may hold values from -0.078125 to 0.078125
Outputs:
- layer_out: bfloat16 [24576, 2048], P(('sp', 'tp'))
The draws below stay inside these ranges and needn't reach their ends.
All inputs are finite; a program needn't handle non-finite values.
Results may differ from the reference program's by a relative error of at most 0.011.
Values may be sent and summed in bfloat16 or wider, within the bound.
No kernel may reach another device: no remote copies, remote signals or barrier semaphores. Data moves between devices by JAX's collectives and lax.ppermute only.
A program may use at most 128 MiB of HBM per device.

```python
import math
import jax
import jax.numpy as jnp
from jax import lax

D = 2048
HEADS = 8
DK = 64
DV = 128
FF = 5632
CONV = 3
BLOCK = 64
TOK_DEV = 768
KW = 512
VW = 1024
TOKENS = 24576


def draw_retention_preactivations(key, part):
    keys_all = jax.random.split(jax.random.fold_in(key, 11), 3)
    ranking = jax.random.permutation(keys_all[0], HEADS)
    fast_count = HEADS // 2
    channel_head = jnp.arange(HEADS * DK) // DK
    head_fast = (ranking < fast_count).astype(jnp.float32)
    chan_fast = jnp.sum((channel_head[:, None] == jnp.arange(HEADS)[None, :]).astype(jnp.float32) * head_fast[None, :], axis=1)
    slow_base = math.log(TOKENS) - 1.6
    base = chan_fast + (1.0 - chan_fast) * slow_base
    device_count = TOKENS // TOK_DEV
    shifts = jax.random.uniform(keys_all[1], (device_count,), jnp.float32, -1.0, 1.0)
    position_dev = jnp.arange(TOKENS) // TOK_DEV
    shift_rows = jnp.sum((position_dev[:, None] == jnp.arange(device_count)[None, :]).astype(jnp.float32) * shifts[None, :], axis=1)
    noise = jnp.clip(jax.random.normal(keys_all[2], (TOKENS, HEADS * DK), jnp.float32), -5.0, 5.0)
    return (base[None, :] + shift_rows[:, None] + noise).astype(jnp.bfloat16)


def draw_additional_fading_amount(key, part):
    keys_all = jax.random.split(jax.random.fold_in(key, 23), 2)
    places = jax.random.randint(keys_all[0], (3,), 0, TOKENS)
    depths = jnp.log(jax.random.uniform(keys_all[1], (3,), jnp.float32, 0.5, 0.8))
    marks = (jnp.arange(TOKENS)[:, None] == places[None, :]).astype(jnp.float32)
    return jnp.sum(marks * depths[None, :], axis=1).astype(jnp.float32)


def levels(key, extent, shards, low, top_value):
    level = 1.0
    for position, parts in shards:
        steps = jax.random.uniform(jax.random.fold_in(jax.random.fold_in(key, 6), position), (parts,), jnp.float32, low / len(shards), top_value / len(shards))
        level = level * jnp.repeat(jnp.exp(steps), extent[position] // parts).reshape((-1,) + (1,) * (len(extent) - 1 - position))
    return level


def normal_values(stream_key, shape, scale, reach, pieces=(), kind=jnp.bfloat16):
    entries = jax.random.normal(stream_key, shape, jnp.float32) * scale
    if len(pieces) > 0:
        entries = levels(stream_key, shape, pieces, -0.22, 0.18) * entries
    return jnp.clip(entries, min=-reach, max=reach).astype(kind)


def setup_inputs(seed: int = 0) -> dict:
    seeds = jax.random.split(jax.random.key(seed), 16)
    residual_input_stream = normal_values(seeds[0], (TOKENS, D), 1.0, 6.0, ((0, 32),))
    projected_queries = normal_values(seeds[1], (TOKENS, KW), 1.0, 6.0, ((0, 32), (1, 4)))
    projected_keys = normal_values(seeds[2], (TOKENS, KW), 1.0, 6.0, ((0, 32), (1, 4)))
    projected_values = normal_values(seeds[3], (TOKENS, VW), 1.0, 6.0, ((0, 32), (1, 4)))
    emitted_switch_entries = normal_values(seeds[4], (TOKENS, VW), 1.0, 6.0, ((0, 32), (1, 4)))
    retention_preactivations = draw_retention_preactivations(jax.random.fold_in(seeds[15], 71), 0)
    additional_fading_amount = draw_additional_fading_amount(jax.random.fold_in(seeds[15], 71), 0)
    head_norm_gain = jnp.clip(1.0 + 0.18 * jax.random.normal(seeds[7], (DV,), jnp.float32), 0.1, 1.9)
    attention_output_weight = normal_values(seeds[8], (VW, D), VW ** -0.5, 0.1875, ((0, 4),))
    feedforward_norm_gain = jnp.clip(1.0 + 0.18 * jax.random.normal(seeds[9], (D,), jnp.float32), 0.1, 1.9)
    gate_up_matrix = normal_values(seeds[10], (D, FF), D ** -0.5, 0.125, ((0, 32), (1, 4)))
    value_up_matrix = normal_values(seeds[11], (D, FF), D ** -0.5, 0.125, ((0, 32), (1, 4)))
    gate_filter_taps = normal_values(seeds[12], (CONV, FF), CONV ** -0.5, 3.5, ((1, 4),))
    value_filter_taps = normal_values(seeds[13], (CONV, FF), CONV ** -0.5, 3.5, ((1, 4),))
    down_projection_weight = normal_values(seeds[14], (FF, D), FF ** -0.5, 0.078125, ((0, 4), (1, 32)))
    return dict(residual_input_stream=residual_input_stream, projected_queries=projected_queries, projected_keys=projected_keys, projected_values=projected_values, emitted_switch_entries=emitted_switch_entries, retention_preactivations=retention_preactivations, additional_fading_amount=additional_fading_amount, head_norm_gain=head_norm_gain, attention_output_weight=attention_output_weight, feedforward_norm_gain=feedforward_norm_gain, gate_up_matrix=gate_up_matrix, value_up_matrix=value_up_matrix, gate_filter_taps=gate_filter_taps, value_filter_taps=value_filter_taps, down_projection_weight=down_projection_weight)


eps = 1e-06
retention_sharpness = 16.0

def to_blocks(tensor, width):
    count = tensor.shape[0] // BLOCK
    return tensor.astype(jnp.float32).reshape(count, BLOCK, HEADS, width)

def depthwise(upward, taps):
    length = upward.shape[0]
    padded = jnp.concatenate([jnp.zeros((CONV - 1, upward.shape[1]), jnp.bfloat16), upward], axis=0)
    result = jnp.zeros(upward.shape, jnp.float32)
    for offset in range(CONV):
        result = result + taps[offset].astype(jnp.float32)[None] * padded[offset:offset + length].astype(jnp.float32)
    return result

def reference(residual_input_stream, projected_queries, projected_keys, projected_values, emitted_switch_entries, retention_preactivations, additional_fading_amount, head_norm_gain, attention_output_weight, feedforward_norm_gain, gate_up_matrix, value_up_matrix, gate_filter_taps, value_filter_taps, down_projection_weight):
    largest_exponent = lax.Precision.HIGHEST
    retention_logarithm = jax.nn.log_sigmoid(retention_preactivations.astype(jnp.float32)) / retention_sharpness + additional_fading_amount[:, None]
    scaled_q = to_blocks(projected_queries, DK) * DK ** (-0.5)
    key_heads = to_blocks(projected_keys, DK)
    value_heads = to_blocks(projected_values, DV)
    rate_cum = jnp.cumsum(to_blocks(retention_logarithm, DK), axis=1)
    block_total = rate_cum[:, -1]
    q_decayed = scaled_q * jnp.exp(rate_cum)
    k_growth = key_heads * jnp.exp(-rate_cum)
    fading_through_finish = key_heads * jnp.exp(block_total[:, None] - rate_cum)
    lower = jnp.tril(jnp.ones((BLOCK, BLOCK), bool))
    scores = jnp.einsum('nihk,njhk->nhij', q_decayed, k_growth, precision=largest_exponent)
    scores = jnp.where(lower[None, None], scores, 0.0)
    within = jnp.einsum('nhij,njhv->nihv', scores, value_heads, precision=largest_exponent)
    increments = jnp.einsum('nchk,nchv->nhkv', fading_through_finish, value_heads, precision=largest_exponent)

    def advance_recurrence(state, inputs):
        factor, increment = inputs
        return (factor[..., None] * state + increment, state)
    start_state = jnp.zeros((HEADS, DK, DV), jnp.float32)
    final_state, state_before = lax.scan(advance_recurrence, start_state, (jnp.exp(block_total), increments))
    earlier = jnp.einsum('nchk,nhkv->nchv', q_decayed, state_before, precision=largest_exponent)
    mech_out = (within + earlier).reshape(TOKENS, HEADS, DV)
    mech_out = mech_out * lax.rsqrt(lax.optimization_barrier(jnp.mean(mech_out * mech_out, axis=-1, keepdims=True)) + eps) * head_norm_gain
    mixed = (mech_out.reshape(TOKENS, VW) * jax.nn.silu(emitted_switch_entries.astype(jnp.float32))).astype(jnp.bfloat16)
    attended = jnp.dot(mixed, attention_output_weight, preferred_element_type=jnp.float32)
    resid = residual_input_stream.astype(jnp.float32) + attended
    normed = (resid * lax.rsqrt(lax.optimization_barrier(jnp.mean(resid * resid, axis=-1, keepdims=True)) + eps) * feedforward_norm_gain).astype(jnp.bfloat16)
    gate_up = jnp.dot(normed, gate_up_matrix, preferred_element_type=jnp.float32).astype(jnp.bfloat16)
    value_up = jnp.dot(normed, value_up_matrix, preferred_element_type=jnp.float32).astype(jnp.bfloat16)
    gate_mix = depthwise(gate_up, gate_filter_taps)
    value_mix = depthwise(value_up, value_filter_taps)
    hidden = (jax.nn.silu(gate_mix) * value_mix).astype(jnp.bfloat16)
    return (resid + jnp.dot(hidden, down_projection_weight, preferred_element_type=jnp.float32)).astype(jnp.bfloat16)
```

```python
import functools
import jax
import jax.numpy as jnp
from jax import lax
from jax.experimental import pallas as pl
from jax.experimental.pallas import tpu as pltpu
from jax.sharding import Mesh
from jax.sharding import PartitionSpec as P

DK = 64
DV = 128
BLOCK = 64
TOK = 768
D = 2048
HID = 1408
HALO = 16
Z, Y, C, X = "z", "y", "c", "x"
SP = (Z, Y, C)
EPS = 1e-06
f32 = jnp.float32
bf16 = jnp.bfloat16
NT = (((1,), (1,)), ((), ()))
TN = (((0,), (0,)), ((), ()))
PACK = 136
VMEM = pl.BlockSpec(memory_space=pltpu.VMEM)


def _params(mib=40, sem=None):
    return pltpu.CompilerParams(vmem_limit_bytes=mib * 1024 * 1024, dimension_semantics=sem)


def _cost(flops, nbytes, trans=0):
    return pl.CostEstimate(flops=int(flops), bytes_accessed=int(nbytes), transcendentals=int(trans))


def _dot(a, b, dims=None):
    if dims is None:
        dims = (((1,), (0,)), ((), ()))
    return lax.dot_general(a, b, dims, preferred_element_type=f32)


def _log_sigmoid(x):
    return jnp.minimum(x, 0.0) - jnp.log1p(jnp.exp(-jnp.abs(x)))


def _silu(x):
    return x / (1.0 + jnp.exp(-x))


def _first_head():
    return lax.broadcasted_iota(jnp.int32, (1, 2 * DK), 1) < DK


def state_kernel(pre_ref, fade_ref, k_ref, v_ref, cum_ref, pack_ref, kf_ref):
    row = lax.broadcasted_iota(jnp.int32, (128, 128), 0)
    col = lax.broadcasted_iota(jnp.int32, (128, 128), 1)
    lower = ((row >= col) & ((row < BLOCK) == (col < BLOCK))).astype(f32)
    ones = jnp.ones((128, 128), f32)
    high = lax.Precision.HIGHEST
    cums = []
    for n in range(TOK // 128):
        rows = slice(n * 128, (n + 1) * 128)
        rate = _log_sigmoid(pre_ref[rows, :].astype(f32)) * (1.0 / 16.0)
        cum = jnp.dot(lower, rate, precision=high, preferred_element_type=f32)
        cum = cum + jnp.dot(
            lower * fade_ref[n : n + 1, :], ones, precision=high, preferred_element_type=f32
        )
        cum_ref[rows, :] = cum
        cums.append(cum)
    suffix = jnp.zeros((1, 2 * DK), f32)
    for b in reversed(range(TOK // BLOCK)):
        n, half = divmod(b, 2)
        cum = cums[n][half * BLOCK : (half + 1) * BLOCK]
        total = cum[BLOCK - 1 : BLOCK]
        rows = slice(b * BLOCK, (b + 1) * BLOCK)
        kf_ref[rows, :] = (k_ref[rows, :].astype(f32) * jnp.exp(suffix + total - cum)).astype(bf16)
        suffix = suffix + total
    kf = kf_ref[...]
    first = _dot(v_ref[:, :DV], kf, TN)
    second = _dot(v_ref[:, DV:], kf, TN)
    pack_ref[0:128, :] = jnp.where(_first_head(), first, second)
    pack_ref[128:PACK, :] = jnp.broadcast_to(jnp.exp(suffix), (8, 128))


def local_kernel(q_ref, k_ref, v_ref, cum_ref, mech_ref, qs_ref):
    head = _first_head()
    row = lax.broadcasted_iota(jnp.int32, (128, BLOCK), 0)
    col = lax.broadcasted_iota(jnp.int32, (128, BLOCK), 1)
    lower = jnp.where(row < BLOCK, row, row - BLOCK) >= col
    state = jnp.zeros((DV, 2 * DK), f32)
    before = jnp.zeros((1, 2 * DK), f32)
    for b in range(TOK // BLOCK):
        rows = slice(b * BLOCK, (b + 1) * BLOCK)
        cum = cum_ref[rows, :]
        total = cum[BLOCK - 1 : BLOCK]
        q = q_ref[rows, :].astype(f32) * DK**-0.5
        k = k_ref[rows, :].astype(f32)
        qd = q * jnp.exp(cum)
        qs_ref[rows, :] = (q * jnp.exp(cum + before)).astype(bf16)
        both = jnp.concatenate([jnp.where(head, qd, 0.0), jnp.where(head, 0.0, qd)], 0).astype(bf16)
        grown = (k * jnp.exp(-cum)).astype(bf16)
        faded = (k * jnp.exp(total - cum)).astype(bf16)
        scores = _dot(both, grown, NT)
        scores = jnp.where(lower, scores, 0.0).astype(bf16)
        inter = _dot(both, state.astype(bf16), NT)
        v0, v1 = v_ref[rows, :DV], v_ref[rows, DV:]
        mech_ref[rows, :DV] = _dot(scores[:BLOCK], v0) + inter[:BLOCK]
        mech_ref[rows, DV:] = _dot(scores[BLOCK:], v1) + inter[BLOCK:]
        update = jnp.where(head, _dot(v0, faded, TN), _dot(v1, faded, TN))
        state = state * jnp.exp(total) + update
        before = before + total


def chip_kernel(own_ref, other_ref, chip_ref):
    second = lax.axis_index(C) == 1
    own_s, own_d = own_ref[0:128, :], own_ref[128:PACK, :]
    oth_s, oth_d = other_ref[0:128, :], other_ref[128:PACK, :]
    s = jnp.where(second, own_d[0:1] * oth_s + own_s, oth_d[0:1] * own_s + oth_s)
    chip_ref[0:128, :] = s
    chip_ref[128:PACK, :] = own_d * oth_d


def plane_kernel(own_ref, up_ref, opp_ref, down_ref, total_ref, before_ref, held):
    y = lax.axis_index(Y)
    held[0] = own_ref[...]
    held[1] = up_ref[...]
    held[2] = opp_ref[...]
    held[3] = down_ref[...]
    s = jnp.zeros((128, 128), f32)
    d = jnp.ones((8, 128), f32)
    before_ref[0:128, :] = s
    before_ref[128:PACK, :] = d
    for k in range(4):
        if k > 0:

            @pl.when(y == k)
            def _(s=s, d=d):
                before_ref[0:128, :] = s
                before_ref[128:PACK, :] = d

        piece = held[lax.rem(k - y + 4, 4)]
        s = piece[128:129] * s + piece[0:128]
        d = piece[128:PACK] * d
    total_ref[0:128, :] = s
    total_ref[128:PACK, :] = d


def finish_kernel(
    mech_ref, qs_ref, z1_ref, z2_ref, z3_ref, yb_ref, other_ref, gate_ref, gain_ref, out_ref
):
    s = z3_ref[0:128, :]
    s = z2_ref[128:129, :] * s + z2_ref[0:128, :]
    s = z1_ref[128:129, :] * s + z1_ref[0:128, :]
    s = yb_ref[128:129, :] * s + yb_ref[0:128, :]
    s = jnp.where(lax.axis_index(C) == 1, other_ref[128:129, :] * s + other_ref[0:128, :], s)
    head = _first_head()
    s0 = jnp.where(head, s, 0.0).astype(bf16)
    s1 = jnp.where(head, 0.0, s).astype(bf16)
    gain = gain_ref[...]
    for n in range(TOK // 128):
        rows = slice(n * 128, (n + 1) * 128)
        for h, sh in enumerate((s0, s1)):
            cols = slice(h * DV, (h + 1) * DV)
            o = mech_ref[rows, cols] + _dot(qs_ref[rows, :], sh, NT)
            o = o * lax.rsqrt(jnp.mean(o * o, axis=-1, keepdims=True) + EPS) * gain
            out_ref[rows, cols] = (o * _silu(gate_ref[rows, cols].astype(f32))).astype(bf16)


ROWS = TOK // 4


def attend_kernel(
    m0, m1, m2, m3, own_w, got1, got2, got3, sib1, sib2, sib3, x_ref, gain_ref,
    normed_ref, resid_ref, w_ref,
):
    c = lax.axis_index(C)
    mine = pl.multiple_of(c * 128, 128)
    theirs = pl.multiple_of((1 - c) * 128, 128)
    w_ref[0] = own_w[...]
    for j, (got, sib) in enumerate(((got1, sib1), (got2, sib2), (got3, sib3))):
        w_ref[j + 1, pl.ds(mine, 128), :] = got[...]
        w_ref[j + 1, pl.ds(theirs, 128), :] = sib[...]
    gain = gain_ref[...]
    xi = lax.axis_index(X)
    for n in range(4):
        rows = slice(n * ROWS, (n + 1) * ROWS)
        acc = x_ref[rows, :].astype(f32)
        for j, m in enumerate((m0, m1, m2, m3)):
            acc = acc + _dot(m[rows, :], w_ref[j])

        @pl.when(xi == n)
        def _(acc=acc):
            resid_ref[...] = acc

        scaled = acc * lax.rsqrt(jnp.mean(acc * acc, axis=-1, keepdims=True) + EPS)
        normed_ref[rows, :] = (scaled * gain).astype(bf16)


def up_kernel(x_ref, halo_ref, wg_ref, wv_ref, tg_ref, tv_ref, out_ref, g_ref):
    w = jnp.concatenate([wg_ref[...].reshape(D, 128), wv_ref[...].reshape(D, 128)], axis=1)
    g_ref[0:HALO, :] = _dot(halo_ref[...], w).astype(bf16).astype(f32)
    for n in range(3):
        at = n * 256
        g_ref[HALO + at : HALO + at + 256, :] = _dot(x_ref[at : at + 256, :], w).astype(bf16).astype(f32)
    taps = jnp.concatenate([tg_ref[...], tv_ref[...]], axis=1).astype(f32)
    for n in range(12):
        at = n * 64
        mix = taps[0:1] * g_ref[HALO - 2 + at : HALO - 2 + at + 64, :]
        mix = mix + taps[1:2] * g_ref[HALO - 1 + at : HALO - 1 + at + 64, :]
        mix = mix + taps[2:3] * g_ref[HALO + at : HALO + at + 64, :]
        out_ref[at : at + 64, :] = (_silu(mix[:, :128]) * mix[:, 128:]).astype(bf16)


def down_kernel(rels, h_ref, w_ref, *out_refs):
    xi = lax.axis_index(X)
    w = w_ref[...].reshape(512, HID)
    for rel, out_ref in zip(rels, out_refs):
        at = pl.multiple_of(lax.rem(xi + rel, 4) * ROWS, ROWS)
        out_ref[...] = _dot(h_ref[pl.ds(at, ROWS), :], w, NT).astype(out_ref.dtype)


def add_kernel(p_ref, ap_ref, m_ref, am_ref, out_p, out_m):
    out_p[...] = (p_ref[...] + ap_ref[...].astype(f32)).astype(bf16)
    out_m[...] = (m_ref[...] + am_ref[...].astype(f32)).astype(bf16)


def last_kernel(resid_ref, own_ref, l_a, l_b, r_a, r_b, out_ref):
    out = resid_ref[:, :1024] + (own_ref[:, :1024] + l_a[...].astype(f32) + r_a[...].astype(f32))
    out_ref[:, :1024] = out.astype(bf16)
    out = resid_ref[:, 1024:] + (own_ref[:, 1024:] + l_b[...].astype(f32) + r_b[...].astype(f32))
    out_ref[:, 1024:] = out.astype(bf16)


def ring(step):
    return [(i, (i + step) % 4) for i in range(4)]


def shape(*dims, dtype=bf16):
    return jax.ShapeDtypeStruct(dims, dtype)


def call(kernel, out_shape, n_in, name, cost, scratch=(), mib=40):
    out_specs = jax.tree.map(lambda _: VMEM, out_shape)
    return pl.pallas_call(
        kernel,
        out_shape=out_shape,
        in_specs=[VMEM] * n_in,
        out_specs=out_specs,
        scratch_shapes=list(scratch),
        compiler_params=_params(mib),
        cost_estimate=cost,
        name=name,
    )


def down(hidden, weights, rels, half, dtype, columns):
    first = half * 2
    blocks = columns // 512
    return pl.pallas_call(
        functools.partial(down_kernel, rels),
        grid=(blocks,),
        out_shape=[shape(ROWS, columns, dtype=dtype) for _ in rels],
        in_specs=[
            pl.BlockSpec((TOK, HID), lambda n: (0, 0)),
            pl.BlockSpec((8, 64, HID), lambda n: (n + first, 2, 0)),
        ],
        out_specs=[pl.BlockSpec((ROWS, 512), lambda n: (0, n)) for _ in rels],
        compiler_params=_params(24, ("arbitrary",)),
        cost_estimate=_cost(2 * ROWS * HID * columns * len(rels), columns * HID * 2 + TOK * HID * 2),
        name="down",
    )(hidden, weights)


def per_device(
    x, q, k, v, switch, pre, fade, head_gain, w_out, ff_gain, w_gate, w_value, t_gate, t_value, w_down
):
    c = lax.axis_index(C)
    packed = jnp.concatenate([w_gate, w_value, w_down.T], axis=0)
    weights = lax.all_gather(packed, SP, axis=0)

    cum, pack = call(
        state_kernel,
        (shape(TOK, 128, dtype=f32), shape(PACK, 128, dtype=f32)),
        4, "state", _cost(2 * TOK * 128 * 256, 1e6), [pltpu.VMEM((TOK, 128), bf16)],
    )(pre, fade.reshape(6, 128), k, v)
    other = lax.ppermute(pack, C, [(0, 1), (1, 0)])

    w_half = lax.dynamic_slice_in_dim(w_out, c * 128, 128, 0)
    w_got = [lax.ppermute(w_half, X, ring(s)) for s in (1, 3, 2)]
    w_sib = [lax.ppermute(w, C, [(0, 1), (1, 0)]) for w in w_got]

    chip = call(chip_kernel, shape(PACK, 128, dtype=f32), 2, "chip", _cost(1e5, 2e5))(pack, other)
    along_y = [lax.ppermute(chip, Y, ring(s)) for s in (3, 2, 1)]
    mech, q_shard = call(
        local_kernel, (shape(TOK, 256, dtype=f32), shape(TOK, 128)), 4, "local",
        _cost(12 * 2 * 128 * 128 * 64 * 8, 3e6),
    )(q, k, v, cum)
    plane, before = call(
        plane_kernel, (shape(PACK, 128, dtype=f32), shape(PACK, 128, dtype=f32)), 4, "plane",
        _cost(1e5, 4e5), [pltpu.VMEM((4, PACK, 128), f32)],
    )(chip, *along_y)
    along_z = [
        lax.ppermute(plane, Z, [(i, i + s) for i in range(4 - s)]) for s in (1, 2, 3)
    ]
    mixed = call(
        finish_kernel, shape(TOK, 256), 9, "finish", _cost(2 * TOK * 128 * 256, 3e6)
    )(mech, q_shard, *along_z, before, other, switch, head_gain.reshape(1, DV))

    mixed_got = [lax.ppermute(mixed, X, ring(s)) for s in (1, 3, 2)]
    normed, resid = call(
        attend_kernel, (shape(TOK, D), shape(ROWS, D, dtype=f32)), 13, "attend",
        _cost(2 * TOK * 1024 * D, 1.2e7), [pltpu.VMEM((4, 256, D), bf16)],
    )(mixed, *mixed_got, w_out, *w_got, *w_sib, x, ff_gain.reshape(1, D))
    halo = lax.ppermute(normed[TOK - HALO :], SP, [(i, i + 1) for i in range(31)])

    hidden = pl.pallas_call(
        up_kernel,
        grid=(HID // 128,),
        out_shape=shape(TOK, HID),
        in_specs=[
            pl.BlockSpec((TOK, D), lambda n: (0, 0)),
            pl.BlockSpec((HALO, D), lambda n: (0, 0)),
            pl.BlockSpec((32, 64, 128), lambda n: (0, 0, n)),
            pl.BlockSpec((32, 64, 128), lambda n: (0, 1, n)),
            pl.BlockSpec((3, 128), lambda n: (0, n)),
            pl.BlockSpec((3, 128), lambda n: (0, n)),
        ],
        out_specs=pl.BlockSpec((TOK, 128), lambda n: (0, n)),
        scratch_shapes=[pltpu.VMEM((HALO + TOK, 256), f32)],
        compiler_params=_params(40, ("arbitrary",)),
        cost_estimate=_cost(2 * TOK * D * 2 * HID, 2 * D * HID * 2 + TOK * D * 2),
        name="up",
    )(normed, halo, weights, weights, t_gate, t_value)

    part = functools.partial(down, hidden, weights)
    (opp_a,) = part((2,), 0, bf16, 1024)
    far_r = lax.ppermute(opp_a, X, ring(1))
    (opp_b,) = part((2,), 1, bf16, 1024)
    far_l = lax.ppermute(opp_b, X, ring(3))
    (next_b,) = part((1,), 1, bf16, 1024)
    near_l_b = lax.ppermute(next_b, X, ring(1))
    (prev_a,) = part((3,), 0, bf16, 1024)
    near_r_a = lax.ppermute(prev_a, X, ring(3))
    (next_a,) = part((1,), 0, f32, 1024)
    (prev_b,) = part((3,), 1, f32, 1024)
    (own,) = part((0,), 0, f32, 2048)
    send_r, send_l = call(
        add_kernel, (shape(ROWS, 1024), shape(ROWS, 1024)), 4, "add", _cost(4e5, 4e6)
    )(next_a, far_r, prev_b, far_l)
    near_l_a = lax.ppermute(send_r, X, ring(1))
    near_r_b = lax.ppermute(send_l, X, ring(3))
    return call(last_kernel, shape(ROWS, D), 6, "last", _cost(1e6, 5e6))(
        resid, own, near_l_a, near_l_b, near_r_a, near_r_b
    )


def solution(mesh):
    torus = Mesh(mesh.devices.reshape(4, 4, 2, 4), (Z, Y, C, X))
    return jax.shard_map(
        per_device,
        mesh=torus,
        in_specs=(
            P(SP, None), P(SP, X), P(SP, X), P(SP, X), P(SP, X), P(SP, X), P(SP), P(),
            P(X, None), P(), P(SP, X), P(SP, X), P(None, X), P(None, X), P(X, SP),
        ),
        out_specs=P((Z, Y, C, X), None),
        check_vma=False,
    )
```

```python
import functools
import jax
import jax.numpy as jnp
from jax import lax
from jax.experimental import pallas as pl
from jax.experimental.pallas import tpu as pltpu
from jax.sharding import Mesh
from jax.sharding import PartitionSpec as P


DK = 64
DV = 128
BLOCK = 64
TOK = 768
D = 2048
HID = 1408
HALO = 16
Z, Y, C, X = "z", "y", "c", "x"
SP = (Z, Y, C)
EPS = 1e-06
f32 = jnp.float32
bf16 = jnp.bfloat16
NT = (((1,), (1,)), ((), ()))
TN = (((0,), (0,)), ((), ()))
PACK = 136
VMEM = pl.BlockSpec(memory_space=pltpu.VMEM)


def _params(mib=40, sem=None):
    return pltpu.CompilerParams(vmem_limit_bytes=mib * 1024 * 1024, dimension_semantics=sem)


def _cost(flops, nbytes, trans=0):
    return pl.CostEstimate(flops=int(flops), bytes_accessed=int(nbytes), transcendentals=int(trans))


def _dot(a, b, dims=None):
    if dims is None:
        dims = (((1,), (0,)), ((), ()))
    return lax.dot_general(a, b, dims, preferred_element_type=f32)


def _log_sigmoid(x):
    return jnp.minimum(x, 0.0) - jnp.log1p(jnp.exp(-jnp.abs(x)))


def _silu(x):
    return x / (1.0 + jnp.exp(-x))


def _first_head():
    return lax.broadcasted_iota(jnp.int32, (1, 2 * DK), 1) < DK


def state_kernel(
    pre_hbm, fade_hbm, k_hbm, v_hbm, cum_ref, pack_ref, kf_ref, pre_ref, fade_ref, k_ref, v_ref, sems
):
    pairs = ((pre_hbm, pre_ref), (fade_hbm, fade_ref), (k_hbm, k_ref), (v_hbm, v_ref))
    copies = [pltpu.make_async_copy(*pair, sems.at[n]) for n, pair in enumerate(pairs)]
    for copy in copies:
        copy.start()
    for copy in copies:
        copy.wait()
    row = lax.broadcasted_iota(jnp.int32, (128, 128), 0)
    col = lax.broadcasted_iota(jnp.int32, (128, 128), 1)
    lower = ((row >= col) & ((row < BLOCK) == (col < BLOCK))).astype(f32)
    ones = jnp.ones((128, 128), f32)
    high = lax.Precision.HIGHEST
    cums = []
    for n in range(TOK // 128):
        rows = slice(n * 128, (n + 1) * 128)
        rate = _log_sigmoid(pre_ref[rows, :].astype(f32)) * (1.0 / 16.0)
        cum = jnp.dot(lower, rate, precision=high, preferred_element_type=f32)
        cum = cum + jnp.dot(
            lower * fade_ref[n : n + 1, :], ones, precision=high, preferred_element_type=f32
        )
        cum_ref[rows, :] = cum
        cums.append(cum)
    suffix = jnp.zeros((1, 2 * DK), f32)
    for b in reversed(range(TOK // BLOCK)):
        n, half = divmod(b, 2)
        cum = cums[n][half * BLOCK : (half + 1) * BLOCK]
        total = cum[BLOCK - 1 : BLOCK]
        rows = slice(b * BLOCK, (b + 1) * BLOCK)
        kf_ref[rows, :] = (k_ref[rows, :].astype(f32) * jnp.exp(suffix + total - cum)).astype(bf16)
        suffix = suffix + total
    kf = kf_ref[...]
    first = _dot(v_ref[:, :DV], kf, TN)
    second = _dot(v_ref[:, DV:], kf, TN)
    pack_ref[0:128, :] = jnp.where(_first_head(), first, second)
    pack_ref[128:PACK, :] = jnp.broadcast_to(jnp.exp(suffix), (8, 128))


def local_kernel(q_ref, k_ref, v_ref, cum_ref, mech_ref, qs_ref):
    head = _first_head()
    row = lax.broadcasted_iota(jnp.int32, (128, BLOCK), 0)
    col = lax.broadcasted_iota(jnp.int32, (128, BLOCK), 1)
    lower = jnp.where(row < BLOCK, row, row - BLOCK) >= col
    state = jnp.zeros((DV, 2 * DK), f32)
    before = jnp.zeros((1, 2 * DK), f32)
    for b in range(TOK // BLOCK):
        rows = slice(b * BLOCK, (b + 1) * BLOCK)
        cum = cum_ref[rows, :]
        total = cum[BLOCK - 1 : BLOCK]
        q = q_ref[rows, :].astype(f32) * DK**-0.5
        k = k_ref[rows, :].astype(f32)
        qd = q * jnp.exp(cum)
        qs_ref[rows, :] = (q * jnp.exp(cum + before)).astype(bf16)
        both = jnp.concatenate([jnp.where(head, qd, 0.0), jnp.where(head, 0.0, qd)], 0).astype(bf16)
        grown = (k * jnp.exp(-cum)).astype(bf16)
        faded = (k * jnp.exp(total - cum)).astype(bf16)
        scores = _dot(both, grown, NT)
        scores = jnp.where(lower, scores, 0.0).astype(bf16)
        inter = _dot(both, state.astype(bf16), NT)
        v0, v1 = v_ref[rows, :DV], v_ref[rows, DV:]
        mech_ref[rows, :DV] = _dot(scores[:BLOCK], v0) + inter[:BLOCK]
        mech_ref[rows, DV:] = _dot(scores[BLOCK:], v1) + inter[BLOCK:]
        update = jnp.where(head, _dot(v0, faded, TN), _dot(v1, faded, TN))
        state = state * jnp.exp(total) + update
        before = before + total


def chip_kernel(own_ref, other_ref, chip_ref):
    second = lax.axis_index(C) == 1
    own_s, own_d = own_ref[0:128, :], own_ref[128:PACK, :]
    oth_s, oth_d = other_ref[0:128, :], other_ref[128:PACK, :]
    s = jnp.where(second, own_d[0:1] * oth_s + own_s, oth_d[0:1] * own_s + oth_s)
    chip_ref[0:128, :] = s
    chip_ref[128:PACK, :] = own_d * oth_d


def plane_kernel(own_ref, up_ref, opp_ref, down_ref, total_ref, before_ref, held):
    y = lax.axis_index(Y)
    held[0] = own_ref[...]
    held[1] = up_ref[...]
    held[2] = opp_ref[...]
    held[3] = down_ref[...]
    s = jnp.zeros((128, 128), f32)
    d = jnp.ones((8, 128), f32)
    before_ref[0:128, :] = s
    before_ref[128:PACK, :] = d
    for k in range(4):
        if k > 0:

            @pl.when(y == k)
            def _(s=s, d=d):
                before_ref[0:128, :] = s
                before_ref[128:PACK, :] = d

        piece = held[lax.rem(k - y + 4, 4)]
        s = piece[128:129] * s + piece[0:128]
        d = piece[128:PACK] * d
    total_ref[0:128, :] = s
    total_ref[128:PACK, :] = d


def enter_kernel(z1_ref, z2_ref, z3_ref, yb_ref, out_ref):
    s = z3_ref[0:128, :]
    s = z2_ref[128:129, :] * s + z2_ref[0:128, :]
    s = z1_ref[128:129, :] * s + z1_ref[0:128, :]
    out_ref[...] = yb_ref[128:129, :] * s + yb_ref[0:128, :]


def finish_kernel(mech_ref, qs_ref, mine_ref, given_ref, other_ref, gate_ref, gain_ref, out_ref):
    given = given_ref[...]
    s = jnp.where(
        lax.axis_index(C) == 1, other_ref[128:129, :] * given + other_ref[0:128, :], mine_ref[...]
    )
    head = _first_head()
    s0 = jnp.where(head, s, 0.0).astype(bf16)
    s1 = jnp.where(head, 0.0, s).astype(bf16)
    gain = gain_ref[...]
    for n in range(TOK // 128):
        rows = slice(n * 128, (n + 1) * 128)
        for h, sh in enumerate((s0, s1)):
            cols = slice(h * DV, (h + 1) * DV)
            o = mech_ref[rows, cols] + _dot(qs_ref[rows, :], sh, NT)
            o = o * lax.rsqrt(jnp.mean(o * o, axis=-1, keepdims=True) + EPS) * gain
            out_ref[rows, cols] = (o * _silu(gate_ref[rows, cols].astype(f32))).astype(bf16)


OFFSETS = (0, 3, 1, 2)
SLOTS = tuple((j, i) for j in range(4) for i in range(4))


def chip_of(core, j, i):
    dz, dy = (i, j) if core == 0 else (j, i)
    z = lax.rem(lax.axis_index(Z) + OFFSETS[dz], 4)
    y = lax.rem(lax.axis_index(Y) + OFFSETS[dy], 4)
    return z * 4 + y


def chip_columns(chip):
    return pl.ds(pl.multiple_of(chip * 128, 128), 128)


def left_half():
    return lax.broadcasted_iota(jnp.int32, (1, 128), 1) < 64


def reorder(src_ref, dst_ref, rows):
    c = lax.axis_index(C)
    left = left_half()
    for core in range(2):
        base = jnp.where(c == core, 0, 1024)
        for t in range(8):
            one = src_ref[:, chip_columns(chip_of(core, *SLOTS[2 * t]))]
            two = src_ref[:, chip_columns(chip_of(core, *SLOTS[2 * t + 1]))]
            if core == 0:
                both = jnp.where(left, one, pltpu.roll(two, 64, 1))
            else:
                both = jnp.where(left, pltpu.roll(one, 64, 1), two)
            at = pl.ds(pl.multiple_of(base + t * 128, 128), 128)
            dst_ref[rows, at] = both.astype(bf16)


ROWS = TOK // 4


def attend_kernel(
    m0, m1, m2, m3, own_w, got1, got2, got3, sib1, sib2, sib3, x_ref, gain_ref,
    *refs,
):
    normed_ref, tail_ref, resid_ref, w_ref, n_ref = refs
    c = lax.axis_index(C)
    mine = pl.multiple_of(c * 128, 128)
    theirs = pl.multiple_of((1 - c) * 128, 128)
    w_ref[0] = own_w[...]
    for j, (got, sib) in enumerate(((got1, sib1), (got2, sib2), (got3, sib3))):
        w_ref[j + 1, pl.ds(mine, 128), :] = got[...]
        w_ref[j + 1, pl.ds(theirs, 128), :] = sib[...]
    gain = gain_ref[...]
    xi = lax.axis_index(X)
    w = w_ref[...].reshape(1024, D)

    def block(n, _):
        rows = pl.ds(pl.multiple_of(n * ROWS, ROWS), ROWS)
        mixed = jnp.concatenate([m[rows, :] for m in (m0, m1, m2, m3)], axis=1)
        acc = x_ref[rows, :].astype(f32) + _dot(mixed, w)

        @pl.when(xi == n)
        def _():
            resid_ref[...] = acc

        scaled = acc * lax.rsqrt(jnp.mean(acc * acc, axis=-1, keepdims=True) + EPS)
        n_ref[...] = scaled * gain

        @pl.when(n == 3)
        def _():
            tail_ref[...] = n_ref[ROWS - HALO :, :].astype(bf16)

        reorder(n_ref, normed_ref, rows)
        return 0

    lax.fori_loop(0, 4, block, 0)


SEG = HALO + ROWS
CHUNKS = tuple((a, min(256, HID - a)) for a in range(0, HID, 256))


def feed_kernel(rels, plan, x_ref, halo_ref, tg_ref, tv_ref, *refs):
    own, sib, refs = refs[:5], refs[5:10], refs[10:]
    out_refs, refs = refs[: len(plan)], refs[len(plan) :]
    xs_ref, hf_ref, hs_ref, g_ref, h_ref = refs
    hf_ref[...] = halo_ref[...].astype(f32)
    reorder(hf_ref, hs_ref, slice(None))
    xi = lax.axis_index(X)
    for s, rel in enumerate(rels):
        block = lax.rem(xi + rel, 4)
        at = pl.multiple_of(block * ROWS, ROWS)
        ahead = pl.multiple_of(jnp.maximum(at - HALO, 0), HALO)
        xs_ref[s * SEG : s * SEG + HALO, :] = jnp.where(
            block == 0, hs_ref[...], x_ref[pl.ds(ahead, HALO), :]
        )
        xs_ref[s * SEG + HALO : (s + 1) * SEG, :] = x_ref[pl.ds(at, ROWS), :]

    def blocks(arrays, part, cols):
        return [w[:, part, :, cols].reshape(w.shape[0] * 64, cols.stop - cols.start) for w in arrays]

    def project(n):
        a, wide = CHUNKS[n]
        for part in range(2):
            cols = slice(a, a + wide)
            w = jnp.concatenate(blocks(own, part, cols) + blocks(sib, part, cols), axis=0)
            new = _dot(xs_ref[...], w).astype(bf16).astype(f32)
            g_ref[n % 2, :, part * 256 : part * 256 + wide] = new

    def mix_columns(n):
        a, wide = CHUNKS[n]
        cols = slice(a, a + wide)
        for s in range(len(rels)):
            r = s * SEG + HALO
            mixes = []
            for part, t_ref in enumerate((tg_ref, tv_ref)):
                taps = t_ref[:, cols].astype(f32)
                at = slice(part * 256, part * 256 + wide)
                mix = taps[0:1] * g_ref[n % 2, r - 2 : r - 2 + ROWS, at]
                mix = mix + taps[1:2] * g_ref[n % 2, r - 1 : r - 1 + ROWS, at]
                mixes.append(mix + taps[2:3] * g_ref[n % 2, r : r + ROWS, at])
            h_ref[s * ROWS : (s + 1) * ROWS, cols] = (_silu(mixes[0]) * mixes[1]).astype(bf16)

    for n in range(len(CHUNKS)):
        project(n)
        if n > 0:
            mix_columns(n - 1)
    mix_columns(len(CHUNKS) - 1)
    for half, arrays in enumerate((own, sib)):
        rows = blocks(arrays, 2, slice(0, HID))
        for n, w in enumerate((rows[:2], rows[2:])):
            new = _dot(h_ref[...], jnp.concatenate(w, axis=0), NT)
            cols = slice(n * 512, n * 512 + 512)
            for (block, want), out_ref in zip(plan, out_refs):
                if want == half:
                    out_ref[:, cols] = new[block * ROWS : (block + 1) * ROWS].astype(out_ref.dtype)


def add_kernel(p_ref, ap_ref, m_ref, am_ref, out_p, out_m):
    out_p[...] = (p_ref[...] + ap_ref[...].astype(f32)).astype(bf16)
    out_m[...] = (m_ref[...] + am_ref[...].astype(f32)).astype(bf16)


def last_kernel(resid_ref, own_a, own_b, l_a, l_b, r_a, r_b, out_ref):
    first = lax.axis_index(C) == 0
    left = left_half()

    def total(g):
        cols = slice(g * 128, (g + 1) * 128)
        a = own_a[:, cols] + l_a[:, cols].astype(f32) + r_a[:, cols].astype(f32)
        b = own_b[:, cols] + l_b[:, cols].astype(f32) + r_b[:, cols].astype(f32)
        return jnp.where(first, a, b), jnp.where(first, b, a)

    totals = [total(g) for g in range(8)]
    for j, i in SLOTS:
        low, high = j * 4 + i, i * 4 + j
        one, two = totals[low // 2][0], totals[high // 2][1]
        one = one if low % 2 == 0 else pltpu.roll(one, 64, 1)
        two = two if high % 2 == 1 else pltpu.roll(two, 64, 1)
        cols = chip_columns(chip_of(0, j, i))
        out_ref[:, cols] = (resid_ref[:, cols] + jnp.where(left, one, two)).astype(bf16)


def by_first_core(along_y, along_z):
    pairs = []
    for z in range(4 - along_z):
        for y in range(4):
            to = (z + along_z) * 4 + (y + along_y) % 4
            pairs.append(((z * 4 + y) * 2, to * 2))
    return pairs


def ring(step):
    return [(i, (i + step) % 4) for i in range(4)]


def shape(*dims, dtype=bf16):
    return jax.ShapeDtypeStruct(dims, dtype)


def call(kernel, out_shape, n_in, cost, scratch=(), mib=8, n_hbm=0):
    out_specs = jax.tree.map(lambda _: VMEM, out_shape)
    return pl.pallas_call(
        kernel,
        out_shape=out_shape,
        in_specs=[VMEM] * n_in + [HBM] * n_hbm,
        out_specs=out_specs,
        scratch_shapes=list(scratch),
        compiler_params=_params(mib),
        cost_estimate=cost,
    )


HBM = pl.BlockSpec(memory_space=pltpu.HBM)
FEED_MIB = 20
ATTEND_MIB = 20


def feed(normed, halo, t_gate, t_value, pieces, rels, plan, dtypes):
    rows = SEG * len(rels)
    return pl.pallas_call(
        functools.partial(feed_kernel, rels, plan),
        out_shape=[shape(ROWS, 1024, dtype=d) for d in dtypes],
        in_specs=[VMEM] * 14,
        out_specs=[VMEM for _ in plan],
        scratch_shapes=[
            pltpu.VMEM((rows, D), bf16),
            pltpu.VMEM((HALO, D), f32),
            pltpu.VMEM((HALO, D), bf16),
            pltpu.VMEM((2, rows, 512), f32),
            pltpu.VMEM((ROWS * len(rels), HID), bf16),
        ],
        compiler_params=_params(FEED_MIB),
        cost_estimate=_cost(2 * rows * D * 3 * HID, 3 * D * HID * 2),
        name="feed",
    )(normed, halo, t_gate, t_value, *pieces)


def around(step, second):
    pairs = []
    for z in range(4):
        for y in range(4):
            for c in range(2):
                along_z = (c == 0) != second
                to = ((z + step) % 4, y, c) if along_z else (z, (y + step) % 4, c)
                pairs.append(((z * 4 + y) * 2 + c, (to[0] * 4 + to[1]) * 2 + c))
    return pairs


def per_device(
    x, q, k, v, switch, pre, fade, head_gain, w_out, ff_gain, w_gate, w_value, t_gate, t_value, w_down
):
    c = lax.axis_index(C)
    swap = [(0, 1), (1, 0)]

    steps = (1, 3, 2)
    shard = jnp.stack([w_gate, w_value, w_down.T], axis=0)
    first = [lax.ppermute(shard, SP, around(s, False)) for s in steps]

    cum, pack = call(
        state_kernel,
        (shape(TOK, 128, dtype=f32), shape(PACK, 128, dtype=f32)),
        0, _cost(2 * TOK * 128 * 256, 1e6),
        [
            pltpu.VMEM((TOK, 128), bf16), pltpu.VMEM((TOK, 128), bf16), pltpu.VMEM((6, 128), f32),
            pltpu.VMEM((TOK, 128), bf16), pltpu.VMEM((TOK, 256), bf16), pltpu.SemaphoreType.DMA((4,)),
        ], 8, 4,
    )(pre, fade.reshape(6, 128), k, v)
    other = lax.ppermute(pack, C, swap)

    w_half = lax.dynamic_slice_in_dim(w_out, c * 128, 128, 0)
    w_got = [lax.ppermute(w_half, X, ring(s)) for s in steps]

    chip = call(chip_kernel, shape(PACK, 128, dtype=f32), 2, _cost(1e5, 2e5))(pack, other)
    along_y = [lax.ppermute(chip, SP, by_first_core(s, 0)) for s in (3, 2, 1)]
    mech, q_shard = call(
        local_kernel, (shape(TOK, 256, dtype=f32), shape(TOK, 128)), 4,
        _cost(12 * 2 * 128 * 128 * 64 * 8, 3e6),
    )(q, k, v, cum)
    plane, before = call(
        plane_kernel, (shape(PACK, 128, dtype=f32), shape(PACK, 128, dtype=f32)), 4,
        _cost(1e5, 4e5), [pltpu.VMEM((4, PACK, 128), f32)],
    )(chip, *along_y)
    along_z = [lax.ppermute(plane, SP, by_first_core(0, s)) for s in (1, 2, 3)]
    entering = call(enter_kernel, shape(128, 128, dtype=f32), 4, _cost(1e5, 3e5))(*along_z, before)
    given = lax.ppermute(entering, C, [(0, 1)])
    stack = jnp.stack([shard, *first], axis=0)
    sides = [lax.ppermute(stack, SP, around(s, True)) for s in (1, 3)]
    mixed = call(
        finish_kernel, shape(TOK, 256), 7, _cost(2 * TOK * 128 * 256, 3e6)
    )(mech, q_shard, entering, given, other, switch, head_gain.reshape(1, DV))

    mixed_got = [lax.ppermute(mixed, X, ring(s)) for s in steps]
    sib_stack = lax.ppermute(stack, C, swap)
    w_sib = [lax.ppermute(w, C, swap) for w in w_got]
    far = [
        lax.ppermute(sides[0][:2], SP, around(1, True)),
        lax.ppermute(sides[1][2:], SP, around(3, True)),
    ]
    sib_sides = [lax.ppermute(w, C, swap) for w in sides]
    normed, tail, resid = call(
        attend_kernel,
        (shape(TOK, D), shape(HALO, D), shape(ROWS, D, dtype=f32)), 13,
        _cost(2 * TOK * 1024 * D, 1.2e7),
        [pltpu.VMEM((4, 256, D), bf16), pltpu.VMEM((ROWS, D), f32)], ATTEND_MIB,
    )(mixed, *mixed_got, w_out, *w_got, *w_sib, x, ff_gain.reshape(1, D))
    halo = lax.ppermute(tail, SP, [(i, i + 1) for i in range(31)])
    sib_far = [lax.ppermute(w, C, swap) for w in far]
    pieces = [stack, *sides, *far, sib_stack, *sib_sides, *sib_far]

    feeds = functools.partial(feed, normed, halo, t_gate, t_value, pieces)
    opp_a, opp_b = feeds((2,), ((0, 0), (0, 1)), (bf16, bf16))
    far_r = lax.ppermute(opp_a, X, ring(1))
    far_l = lax.ppermute(opp_b, X, ring(3))
    next_a, next_b, prev_a, prev_b = feeds(
        (1, 3), ((0, 0), (0, 1), (1, 0), (1, 1)), (f32, bf16, bf16, f32)
    )
    near_l_b = lax.ppermute(next_b, X, ring(1))
    near_r_a = lax.ppermute(prev_a, X, ring(3))
    send_r, send_l = call(
        add_kernel, (shape(ROWS, 1024), shape(ROWS, 1024)), 4, _cost(4e5, 4e6)
    )(next_a, far_r, prev_b, far_l)
    near_l_a = lax.ppermute(send_r, X, ring(1))
    near_r_b = lax.ppermute(send_l, X, ring(3))
    own_a, own_b = feeds((0,), ((0, 0), (0, 1)), (f32, f32))
    return call(last_kernel, shape(ROWS, D), 7, _cost(1e6, 5e6))(
        resid, own_a, own_b, near_l_a, near_l_b, near_r_a, near_r_b
    )


def solution(mesh):
    torus = Mesh(mesh.devices.reshape(4, 4, 2, 4), (Z, Y, C, X))
    return jax.shard_map(
        per_device,
        mesh=torus,
        in_specs=(
            P(SP, None), P(SP, X), P(SP, X), P(SP, X), P(SP, X), P(SP, X), P(SP), P(),
            P(X, None), P(), P(SP, X), P(SP, X), P(None, X), P(None, X), P(X, SP),
        ),
        out_specs=P((Z, Y, C, X), None),
        check_vma=False,
    )
```

```python
import functools
import jax
import jax.numpy as jnp
from jax import lax
from jax.experimental import pallas as pl
from jax.experimental.pallas import tpu as pltpu
from jax.sharding import Mesh
from jax.sharding import PartitionSpec as P


DK = 64
DV = 128
BLOCK = 64
TOK = 768
D = 2048
HID = 1408
HALO = 16
Z, Y, C, X = "z", "y", "c", "x"
SP = (Z, Y, C)
EPS = 1e-06
f32 = jnp.float32
bf16 = jnp.bfloat16
NT = (((1,), (1,)), ((), ()))
TN = (((0,), (0,)), ((), ()))
PACK = 136
VMEM = pl.BlockSpec(memory_space=pltpu.VMEM)


def _params(mib=40, sem=None):
    return pltpu.CompilerParams(vmem_limit_bytes=mib * 1024 * 1024, dimension_semantics=sem)


def _cost(flops, nbytes, trans=0):
    return pl.CostEstimate(flops=int(flops), bytes_accessed=int(nbytes), transcendentals=int(trans))


def _dot(a, b, dims=None):
    if dims is None:
        dims = (((1,), (0,)), ((), ()))
    return lax.dot_general(a, b, dims, preferred_element_type=f32)


def _log_sigmoid(x):
    return jnp.minimum(x, 0.0) - jnp.log1p(jnp.exp(-jnp.abs(x)))


def _silu(x):
    return x / (1.0 + jnp.exp(-x))


def _first_head():
    return lax.broadcasted_iota(jnp.int32, (1, 2 * DK), 1) < DK


def state_kernel(
    pre_hbm, fade_hbm, k_hbm, v_hbm, cum_ref, pack_ref, kf_ref, pre_ref, fade_ref, k_ref, v_ref, sems
):
    pairs = ((pre_hbm, pre_ref), (fade_hbm, fade_ref), (k_hbm, k_ref), (v_hbm, v_ref))
    copies = [pltpu.make_async_copy(*pair, sems.at[n]) for n, pair in enumerate(pairs)]
    for copy in copies:
        copy.start()
    for copy in copies:
        copy.wait()
    row = lax.broadcasted_iota(jnp.int32, (128, 128), 0)
    col = lax.broadcasted_iota(jnp.int32, (128, 128), 1)
    lower = ((row >= col) & ((row < BLOCK) == (col < BLOCK))).astype(f32)
    ones = jnp.ones((128, 128), f32)
    high = lax.Precision.HIGHEST
    cums = []
    for n in range(TOK // 128):
        rows = slice(n * 128, (n + 1) * 128)
        rate = _log_sigmoid(pre_ref[rows, :].astype(f32)) * (1.0 / 16.0)
        cum = jnp.dot(lower, rate, precision=high, preferred_element_type=f32)
        cum = cum + jnp.dot(
            lower * fade_ref[n : n + 1, :], ones, precision=high, preferred_element_type=f32
        )
        cum_ref[rows, :] = cum
        cums.append(cum)
    suffix = jnp.zeros((1, 2 * DK), f32)
    for b in reversed(range(TOK // BLOCK)):
        n, half = divmod(b, 2)
        cum = cums[n][half * BLOCK : (half + 1) * BLOCK]
        total = cum[BLOCK - 1 : BLOCK]
        rows = slice(b * BLOCK, (b + 1) * BLOCK)
        kf_ref[rows, :] = (k_ref[rows, :].astype(f32) * jnp.exp(suffix + total - cum)).astype(bf16)
        suffix = suffix + total
    kf = kf_ref[...]
    first = _dot(v_ref[:, :DV], kf, TN)
    second = _dot(v_ref[:, DV:], kf, TN)
    pack_ref[0:128, :] = jnp.where(_first_head(), first, second)
    pack_ref[128:PACK, :] = jnp.broadcast_to(jnp.exp(suffix), (8, 128))


def local_kernel(q_ref, k_ref, v_ref, cum_ref, mech_ref, qs_ref):
    head = _first_head()
    row = lax.broadcasted_iota(jnp.int32, (128, BLOCK), 0)
    col = lax.broadcasted_iota(jnp.int32, (128, BLOCK), 1)
    lower = jnp.where(row < BLOCK, row, row - BLOCK) >= col
    state = jnp.zeros((DV, 2 * DK), f32)
    before = jnp.zeros((1, 2 * DK), f32)
    for b in range(TOK // BLOCK):
        rows = slice(b * BLOCK, (b + 1) * BLOCK)
        cum = cum_ref[rows, :]
        total = cum[BLOCK - 1 : BLOCK]
        q = q_ref[rows, :].astype(f32) * DK**-0.5
        k = k_ref[rows, :].astype(f32)
        qd = q * jnp.exp(cum)
        qs_ref[rows, :] = (q * jnp.exp(cum + before)).astype(bf16)
        both = jnp.concatenate([jnp.where(head, qd, 0.0), jnp.where(head, 0.0, qd)], 0).astype(bf16)
        grown = (k * jnp.exp(-cum)).astype(bf16)
        faded = (k * jnp.exp(total - cum)).astype(bf16)
        scores = _dot(both, grown, NT)
        scores = jnp.where(lower, scores, 0.0).astype(bf16)
        inter = _dot(both, state.astype(bf16), NT)
        v0, v1 = v_ref[rows, :DV], v_ref[rows, DV:]
        mech_ref[rows, :DV] = _dot(scores[:BLOCK], v0) + inter[:BLOCK]
        mech_ref[rows, DV:] = _dot(scores[BLOCK:], v1) + inter[BLOCK:]
        update = jnp.where(head, _dot(v0, faded, TN), _dot(v1, faded, TN))
        state = state * jnp.exp(total) + update
        before = before + total


def chip_kernel(own_ref, other_ref, chip_ref):
    second = lax.axis_index(C) == 1
    own_s, own_d = own_ref[0:128, :], own_ref[128:PACK, :]
    oth_s, oth_d = other_ref[0:128, :], other_ref[128:PACK, :]
    s = jnp.where(second, own_d[0:1] * oth_s + own_s, oth_d[0:1] * own_s + oth_s)
    chip_ref[0:128, :] = s
    chip_ref[128:PACK, :] = own_d * oth_d


def plane_kernel(own_ref, up_ref, opp_ref, down_ref, total_ref, before_ref, held):
    y = lax.axis_index(Y)
    held[0] = own_ref[...]
    held[1] = up_ref[...]
    held[2] = opp_ref[...]
    held[3] = down_ref[...]
    s = jnp.zeros((128, 128), f32)
    d = jnp.ones((8, 128), f32)
    before_ref[0:128, :] = s
    before_ref[128:PACK, :] = d
    for k in range(4):
        if k > 0:

            @pl.when(y == k)
            def _(s=s, d=d):
                before_ref[0:128, :] = s
                before_ref[128:PACK, :] = d

        piece = held[lax.rem(k - y + 4, 4)]
        s = piece[128:129] * s + piece[0:128]
        d = piece[128:PACK] * d
    total_ref[0:128, :] = s
    total_ref[128:PACK, :] = d


def enter_kernel(z1_ref, z2_ref, z3_ref, yb_ref, out_ref):
    s = z3_ref[0:128, :]
    s = z2_ref[128:129, :] * s + z2_ref[0:128, :]
    s = z1_ref[128:129, :] * s + z1_ref[0:128, :]
    out_ref[...] = yb_ref[128:129, :] * s + yb_ref[0:128, :]


def finish_kernel(mech_ref, qs_ref, mine_ref, given_ref, other_ref, gate_ref, gain_ref, out_ref):
    given = given_ref[...]
    s = jnp.where(
        lax.axis_index(C) == 1, other_ref[128:129, :] * given + other_ref[0:128, :], mine_ref[...]
    )
    head = _first_head()
    s0 = jnp.where(head, s, 0.0).astype(bf16)
    s1 = jnp.where(head, 0.0, s).astype(bf16)
    gain = gain_ref[...]
    for n in range(TOK // 128):
        rows = slice(n * 128, (n + 1) * 128)
        for h, sh in enumerate((s0, s1)):
            cols = slice(h * DV, (h + 1) * DV)
            o = mech_ref[rows, cols] + _dot(qs_ref[rows, :], sh, NT)
            o = o * lax.rsqrt(jnp.mean(o * o, axis=-1, keepdims=True) + EPS) * gain
            out_ref[rows, cols] = (o * _silu(gate_ref[rows, cols].astype(f32))).astype(bf16)


OFFSETS = (0, 3, 1, 2)
SLOTS = tuple((j, i) for j in range(4) for i in range(4))


def chip_of(core, j, i):
    dz, dy = (i, j) if core == 0 else (j, i)
    z = lax.rem(lax.axis_index(Z) + OFFSETS[dz], 4)
    y = lax.rem(lax.axis_index(Y) + OFFSETS[dy], 4)
    return z * 4 + y


def chip_columns(chip):
    return pl.ds(pl.multiple_of(chip * 128, 128), 128)


def left_half():
    return lax.broadcasted_iota(jnp.int32, (1, 128), 1) < 64


def reorder(src_ref, dst_ref, rows):
    c = lax.axis_index(C)
    left = left_half()
    for core in range(2):
        base = jnp.where(c == core, 0, 1024)
        for t in range(8):
            one = src_ref[:, chip_columns(chip_of(core, *SLOTS[2 * t]))]
            two = src_ref[:, chip_columns(chip_of(core, *SLOTS[2 * t + 1]))]
            if core == 0:
                both = jnp.where(left, one, pltpu.roll(two, 64, 1))
            else:
                both = jnp.where(left, pltpu.roll(one, 64, 1), two)
            at = pl.ds(pl.multiple_of(base + t * 128, 128), 128)
            dst_ref[rows, at] = both.astype(bf16)


ROWS = TOK // 4


def attend_kernel(
    m0, m1, m2, m3, own_w, got1, got2, got3, sib1, sib2, sib3, x_ref, gain_ref,
    *refs,
):
    normed_ref, tail_ref, resid_ref, w_ref, n_ref = refs
    c = lax.axis_index(C)
    mine = pl.multiple_of(c * 128, 128)
    theirs = pl.multiple_of((1 - c) * 128, 128)
    w_ref[0] = own_w[...]
    for j, (got, sib) in enumerate(((got1, sib1), (got2, sib2), (got3, sib3))):
        w_ref[j + 1, pl.ds(mine, 128), :] = got[...]
        w_ref[j + 1, pl.ds(theirs, 128), :] = sib[...]
    gain = gain_ref[...]
    xi = lax.axis_index(X)
    w = w_ref[...].reshape(1024, D)

    def block(n, _):
        rows = pl.ds(pl.multiple_of(n * ROWS, ROWS), ROWS)
        mixed = jnp.concatenate([m[rows, :] for m in (m0, m1, m2, m3)], axis=1)
        acc = x_ref[rows, :].astype(f32) + _dot(mixed, w)

        @pl.when(xi == n)
        def _():
            resid_ref[...] = acc

        scaled = acc * lax.rsqrt(jnp.mean(acc * acc, axis=-1, keepdims=True) + EPS)
        n_ref[...] = scaled * gain

        @pl.when(n == 3)
        def _():
            tail_ref[...] = n_ref[ROWS - HALO :, :].astype(bf16)

        reorder(n_ref, normed_ref, rows)
        return 0

    lax.fori_loop(0, 4, block, 0)


SEG = HALO + ROWS
CHUNKS = tuple((a, min(256, HID - a)) for a in range(0, HID, 256))


def feed_kernel(rels, plan, x_ref, halo_ref, tg_ref, tv_ref, *refs):
    own, sib, refs = refs[:5], refs[5:10], refs[10:]
    out_refs, refs = refs[: len(plan)], refs[len(plan) :]
    xs_ref, hf_ref, hs_ref, g_ref, h_ref = refs
    hf_ref[...] = halo_ref[...].astype(f32)
    reorder(hf_ref, hs_ref, slice(None))
    xi = lax.axis_index(X)
    for s, rel in enumerate(rels):
        block = lax.rem(xi + rel, 4)
        at = pl.multiple_of(block * ROWS, ROWS)
        ahead = pl.multiple_of(jnp.maximum(at - HALO, 0), HALO)
        xs_ref[s * SEG : s * SEG + HALO, :] = jnp.where(
            block == 0, hs_ref[...], x_ref[pl.ds(ahead, HALO), :]
        )
        xs_ref[s * SEG + HALO : (s + 1) * SEG, :] = x_ref[pl.ds(at, ROWS), :]

    def blocks(arrays, part, cols):
        return [w[:, part, :, cols].reshape(w.shape[0] * 64, cols.stop - cols.start) for w in arrays]

    def project(n):
        a, wide = CHUNKS[n]
        for part in range(2):
            cols = slice(a, a + wide)
            w = jnp.concatenate(blocks(own, part, cols) + blocks(sib, part, cols), axis=0)
            new = _dot(xs_ref[...], w).astype(bf16).astype(f32)
            g_ref[n % 2, :, part * 256 : part * 256 + wide] = new

    def mix_columns(n):
        a, wide = CHUNKS[n]
        cols = slice(a, a + wide)
        for s in range(len(rels)):
            r = s * SEG + HALO
            mixes = []
            for part, t_ref in enumerate((tg_ref, tv_ref)):
                taps = t_ref[:, cols].astype(f32)
                at = slice(part * 256, part * 256 + wide)
                mix = taps[0:1] * g_ref[n % 2, r - 2 : r - 2 + ROWS, at]
                mix = mix + taps[1:2] * g_ref[n % 2, r - 1 : r - 1 + ROWS, at]
                mixes.append(mix + taps[2:3] * g_ref[n % 2, r : r + ROWS, at])
            h_ref[s * ROWS : (s + 1) * ROWS, cols] = (_silu(mixes[0]) * mixes[1]).astype(bf16)

    for n in range(len(CHUNKS)):
        project(n)
        if n > 0:
            mix_columns(n - 1)
    mix_columns(len(CHUNKS) - 1)
    for half, arrays in enumerate((own, sib)):
        rows = blocks(arrays, 2, slice(0, HID))
        for n, w in enumerate((rows[:2], rows[2:])):
            new = _dot(h_ref[...], jnp.concatenate(w, axis=0), NT)
            cols = slice(n * 512, n * 512 + 512)
            for (block, want), out_ref in zip(plan, out_refs):
                if want == half:
                    out_ref[:, cols] = new[block * ROWS : (block + 1) * ROWS].astype(out_ref.dtype)


def add_kernel(p_ref, ap_ref, m_ref, am_ref, out_p, out_m):
    out_p[...] = (p_ref[...] + ap_ref[...].astype(f32)).astype(bf16)
    out_m[...] = (m_ref[...] + am_ref[...].astype(f32)).astype(bf16)


def last_kernel(resid_ref, own_a, own_b, l_a, l_b, r_a, r_b, out_ref):
    first = lax.axis_index(C) == 0
    left = left_half()

    def total(g):
        cols = slice(g * 128, (g + 1) * 128)
        a = own_a[:, cols] + l_a[:, cols].astype(f32) + r_a[:, cols].astype(f32)
        b = own_b[:, cols] + l_b[:, cols].astype(f32) + r_b[:, cols].astype(f32)
        return jnp.where(first, a, b), jnp.where(first, b, a)

    totals = [total(g) for g in range(8)]
    for j, i in SLOTS:
        low, high = j * 4 + i, i * 4 + j
        one, two = totals[low // 2][0], totals[high // 2][1]
        one = one if low % 2 == 0 else pltpu.roll(one, 64, 1)
        two = two if high % 2 == 1 else pltpu.roll(two, 64, 1)
        cols = chip_columns(chip_of(0, j, i))
        out_ref[:, cols] = (resid_ref[:, cols] + jnp.where(left, one, two)).astype(bf16)


def by_first_core(step):
    pairs = []
    for z in range(4 - step):
        for y in range(4):
            pairs.append(((z * 4 + y) * 2, ((z + step) * 4 + y) * 2))
    return pairs


def ring(step):
    return [(i, (i + step) % 4) for i in range(4)]


def shape(*dims, dtype=bf16):
    return jax.ShapeDtypeStruct(dims, dtype)


def call(kernel, out_shape, n_in, cost, scratch=(), mib=8, n_hbm=0):
    out_specs = jax.tree.map(lambda _: VMEM, out_shape)
    return pl.pallas_call(
        kernel,
        out_shape=out_shape,
        in_specs=[VMEM] * n_in + [HBM] * n_hbm,
        out_specs=out_specs,
        scratch_shapes=list(scratch),
        compiler_params=_params(mib),
        cost_estimate=cost,
    )


HBM = pl.BlockSpec(memory_space=pltpu.HBM)
FEED_MIB = 20
ATTEND_MIB = 20


def feed(normed, halo, t_gate, t_value, pieces, rels, plan, dtypes):
    rows = SEG * len(rels)
    return pl.pallas_call(
        functools.partial(feed_kernel, rels, plan),
        out_shape=[shape(ROWS, 1024, dtype=d) for d in dtypes],
        in_specs=[VMEM] * 14,
        out_specs=[VMEM for _ in plan],
        scratch_shapes=[
            pltpu.VMEM((rows, D), bf16),
            pltpu.VMEM((HALO, D), f32),
            pltpu.VMEM((HALO, D), bf16),
            pltpu.VMEM((2, rows, 512), f32),
            pltpu.VMEM((ROWS * len(rels), HID), bf16),
        ],
        compiler_params=_params(FEED_MIB),
        cost_estimate=_cost(2 * rows * D * 3 * HID, 3 * D * HID * 2),
        name="feed",
    )(normed, halo, t_gate, t_value, *pieces)


def around(step, second):
    pairs = []
    for z in range(4):
        for y in range(4):
            for c in range(2):
                along_z = (c == 0) != second
                to = ((z + step) % 4, y, c) if along_z else (z, (y + step) % 4, c)
                pairs.append(((z * 4 + y) * 2 + c, (to[0] * 4 + to[1]) * 2 + c))
    return pairs


def per_device(
    x, q, k, v, switch, pre, fade, head_gain, w_out, ff_gain, w_gate, w_value, t_gate, t_value, w_down
):
    c = lax.axis_index(C)
    swap = [(0, 1), (1, 0)]

    steps = (1, 3, 2)
    shard = jnp.stack([w_gate, w_value, w_down.T], axis=0)
    first = [lax.ppermute(shard, SP, around(s, False)) for s in steps]

    cum, pack = call(
        state_kernel,
        (shape(TOK, 128, dtype=f32), shape(PACK, 128, dtype=f32)),
        0, _cost(2 * TOK * 128 * 256, 1e6),
        [
            pltpu.VMEM((TOK, 128), bf16), pltpu.VMEM((TOK, 128), bf16), pltpu.VMEM((6, 128), f32),
            pltpu.VMEM((TOK, 128), bf16), pltpu.VMEM((TOK, 256), bf16), pltpu.SemaphoreType.DMA((4,)),
        ], 8, 4,
    )(pre, fade.reshape(6, 128), k, v)
    other = lax.ppermute(pack, C, swap)

    w_half = lax.dynamic_slice_in_dim(w_out, c * 128, 128, 0)
    w_got = [lax.ppermute(w_half, X, ring(s)) for s in steps]

    chip = call(chip_kernel, shape(PACK, 128, dtype=f32), 2, _cost(1e5, 2e5))(pack, other)
    along_y = [lax.ppermute(chip, Y, ring(s)) for s in (3, 2, 1)]
    mech, q_shard = call(
        local_kernel, (shape(TOK, 256, dtype=f32), shape(TOK, 128)), 4,
        _cost(12 * 2 * 128 * 128 * 64 * 8, 3e6),
    )(q, k, v, cum)
    plane, before = call(
        plane_kernel, (shape(PACK, 128, dtype=f32), shape(PACK, 128, dtype=f32)), 4,
        _cost(1e5, 4e5), [pltpu.VMEM((4, PACK, 128), f32)],
    )(chip, *along_y)
    along_z = [lax.ppermute(plane, SP, by_first_core(s)) for s in (1, 2, 3)]
    entering = call(enter_kernel, shape(128, 128, dtype=f32), 4, _cost(1e5, 3e5))(*along_z, before)
    given = lax.ppermute(entering, C, [(0, 1)])
    stack = jnp.stack([shard, *first], axis=0)
    sides = [lax.ppermute(stack, SP, around(s, True)) for s in (1, 3)]
    mixed = call(
        finish_kernel, shape(TOK, 256), 7, _cost(2 * TOK * 128 * 256, 3e6)
    )(mech, q_shard, entering, given, other, switch, head_gain.reshape(1, DV))

    mixed_got = [lax.ppermute(mixed, X, ring(s)) for s in steps]
    sib_stack = lax.ppermute(stack, C, swap)
    w_sib = [lax.ppermute(w, C, swap) for w in w_got]
    far = [
        lax.ppermute(sides[0][:2], SP, around(1, True)),
        lax.ppermute(sides[1][2:], SP, around(3, True)),
    ]
    sib_sides = [lax.ppermute(w, C, swap) for w in sides]
    normed, tail, resid = call(
        attend_kernel,
        (shape(TOK, D), shape(HALO, D), shape(ROWS, D, dtype=f32)), 13,
        _cost(2 * TOK * 1024 * D, 1.2e7),
        [pltpu.VMEM((4, 256, D), bf16), pltpu.VMEM((ROWS, D), f32)], ATTEND_MIB,
    )(mixed, *mixed_got, w_out, *w_got, *w_sib, x, ff_gain.reshape(1, D))
    halo = lax.ppermute(tail, SP, [(i, i + 1) for i in range(31)])
    sib_far = [lax.ppermute(w, C, swap) for w in far]
    pieces = [stack, *sides, *far, sib_stack, *sib_sides, *sib_far]

    feeds = functools.partial(feed, normed, halo, t_gate, t_value, pieces)
    opp_a, opp_b = feeds((2,), ((0, 0), (0, 1)), (bf16, bf16))
    far_r = lax.ppermute(opp_a, X, ring(1))
    far_l = lax.ppermute(opp_b, X, ring(3))
    next_a, next_b, prev_a, prev_b = feeds(
        (1, 3), ((0, 0), (0, 1), (1, 0), (1, 1)), (f32, bf16, bf16, f32)
    )
    near_l_b = lax.ppermute(next_b, X, ring(1))
    near_r_a = lax.ppermute(prev_a, X, ring(3))
    send_r, send_l = call(
        add_kernel, (shape(ROWS, 1024), shape(ROWS, 1024)), 4, _cost(4e5, 4e6)
    )(next_a, far_r, prev_b, far_l)
    near_l_a = lax.ppermute(send_r, X, ring(1))
    near_r_b = lax.ppermute(send_l, X, ring(3))
    own_a, own_b = feeds((0,), ((0, 0), (0, 1)), (f32, f32))
    return call(last_kernel, shape(ROWS, D), 7, _cost(1e6, 5e6))(
        resid, own_a, own_b, near_l_a, near_l_b, near_r_a, near_r_b
    )


def solution(mesh):
    torus = Mesh(mesh.devices.reshape(4, 4, 2, 4), (Z, Y, C, X))
    return jax.shard_map(
        per_device,
        mesh=torus,
        in_specs=(
            P(SP, None), P(SP, X), P(SP, X), P(SP, X), P(SP, X), P(SP, X), P(SP), P(),
            P(X, None), P(), P(SP, X), P(SP, X), P(None, X), P(None, X), P(X, SP),
        ),
        out_specs=P((Z, Y, C, X), None),
        check_vma=False,
    )
```

```python
import functools
import jax
import jax.numpy as jnp
from jax import lax
from jax.experimental import pallas as pl
from jax.experimental.pallas import tpu as pltpu
from jax.sharding import Mesh
from jax.sharding import PartitionSpec as P


DK = 64
DV = 128
BLOCK = 64
TOK = 768
D = 2048
HID = 1408
HALO = 16
Z, Y, C, X = "z", "y", "c", "x"
SP = (Z, Y, C)
EPS = 1e-06
f32 = jnp.float32
bf16 = jnp.bfloat16
NT = (((1,), (1,)), ((), ()))
TN = (((0,), (0,)), ((), ()))
PACK = 136
VMEM = pl.BlockSpec(memory_space=pltpu.VMEM)


def _params(mib=40, sem=None):
    return pltpu.CompilerParams(vmem_limit_bytes=mib * 1024 * 1024, dimension_semantics=sem)


def _cost(flops, nbytes, trans=0):
    return pl.CostEstimate(flops=int(flops), bytes_accessed=int(nbytes), transcendentals=int(trans))


def _dot(a, b, dims=None):
    if dims is None:
        dims = (((1,), (0,)), ((), ()))
    return lax.dot_general(a, b, dims, preferred_element_type=f32)


def _log_sigmoid(x):
    return jnp.minimum(x, 0.0) - jnp.log1p(jnp.exp(-jnp.abs(x)))


def _silu(x):
    return x / (1.0 + jnp.exp(-x))


def _first_head():
    return lax.broadcasted_iota(jnp.int32, (1, 2 * DK), 1) < DK


def state_kernel(
    pre_hbm, fade_hbm, k_hbm, v_hbm, cum_ref, pack_ref, kf_ref, pre_ref, fade_ref, k_ref, v_ref, sems
):
    pairs = ((pre_hbm, pre_ref), (fade_hbm, fade_ref), (k_hbm, k_ref), (v_hbm, v_ref))
    copies = [pltpu.make_async_copy(*pair, sems.at[n]) for n, pair in enumerate(pairs)]
    for copy in copies:
        copy.start()
    for copy in copies:
        copy.wait()
    row = lax.broadcasted_iota(jnp.int32, (128, 128), 0)
    col = lax.broadcasted_iota(jnp.int32, (128, 128), 1)
    lower = ((row >= col) & ((row < BLOCK) == (col < BLOCK))).astype(f32)
    ones = jnp.ones((128, 128), f32)
    high = lax.Precision.HIGHEST
    cums = []
    for n in range(TOK // 128):
        rows = slice(n * 128, (n + 1) * 128)
        rate = _log_sigmoid(pre_ref[rows, :].astype(f32)) * (1.0 / 16.0)
        cum = jnp.dot(lower, rate, precision=high, preferred_element_type=f32)
        cum = cum + jnp.dot(
            lower * fade_ref[n : n + 1, :], ones, precision=high, preferred_element_type=f32
        )
        cum_ref[rows, :] = cum
        cums.append(cum)
    suffix = jnp.zeros((1, 2 * DK), f32)
    for b in reversed(range(TOK // BLOCK)):
        n, half = divmod(b, 2)
        cum = cums[n][half * BLOCK : (half + 1) * BLOCK]
        total = cum[BLOCK - 1 : BLOCK]
        rows = slice(b * BLOCK, (b + 1) * BLOCK)
        kf_ref[rows, :] = (k_ref[rows, :].astype(f32) * jnp.exp(suffix + total - cum)).astype(bf16)
        suffix = suffix + total
    kf = kf_ref[...]
    first = _dot(v_ref[:, :DV], kf, TN)
    second = _dot(v_ref[:, DV:], kf, TN)
    pack_ref[0:128, :] = jnp.where(_first_head(), first, second)
    pack_ref[128:PACK, :] = jnp.broadcast_to(jnp.exp(suffix), (8, 128))


def local_kernel(q_ref, k_ref, v_ref, cum_ref, mech_ref, qs_ref):
    head = _first_head()
    row = lax.broadcasted_iota(jnp.int32, (128, BLOCK), 0)
    col = lax.broadcasted_iota(jnp.int32, (128, BLOCK), 1)
    lower = jnp.where(row < BLOCK, row, row - BLOCK) >= col
    state = jnp.zeros((DV, 2 * DK), f32)
    before = jnp.zeros((1, 2 * DK), f32)
    for b in range(TOK // BLOCK):
        rows = slice(b * BLOCK, (b + 1) * BLOCK)
        cum = cum_ref[rows, :]
        total = cum[BLOCK - 1 : BLOCK]
        q = q_ref[rows, :].astype(f32) * DK**-0.5
        k = k_ref[rows, :].astype(f32)
        qd = q * jnp.exp(cum)
        qs_ref[rows, :] = (q * jnp.exp(cum + before)).astype(bf16)
        both = jnp.concatenate([jnp.where(head, qd, 0.0), jnp.where(head, 0.0, qd)], 0).astype(bf16)
        grown = (k * jnp.exp(-cum)).astype(bf16)
        faded = (k * jnp.exp(total - cum)).astype(bf16)
        scores = _dot(both, grown, NT)
        scores = jnp.where(lower, scores, 0.0).astype(bf16)
        inter = _dot(both, state.astype(bf16), NT)
        v0, v1 = v_ref[rows, :DV], v_ref[rows, DV:]
        mech_ref[rows, :DV] = _dot(scores[:BLOCK], v0) + inter[:BLOCK]
        mech_ref[rows, DV:] = _dot(scores[BLOCK:], v1) + inter[BLOCK:]
        update = jnp.where(head, _dot(v0, faded, TN), _dot(v1, faded, TN))
        state = state * jnp.exp(total) + update
        before = before + total


def chip_kernel(own_ref, other_ref, chip_ref):
    second = lax.axis_index(C) == 1
    own_s, own_d = own_ref[0:128, :], own_ref[128:PACK, :]
    oth_s, oth_d = other_ref[0:128, :], other_ref[128:PACK, :]
    s = jnp.where(second, own_d[0:1] * oth_s + own_s, oth_d[0:1] * own_s + oth_s)
    chip_ref[0:128, :] = s
    chip_ref[128:PACK, :] = own_d * oth_d


def plane_kernel(own_ref, up_ref, opp_ref, down_ref, total_ref, before_ref, held):
    y = lax.axis_index(Y)
    held[0] = own_ref[...]
    held[1] = up_ref[...]
    held[2] = opp_ref[...]
    held[3] = down_ref[...]
    s = jnp.zeros((128, 128), f32)
    d = jnp.ones((8, 128), f32)
    before_ref[0:128, :] = s
    before_ref[128:PACK, :] = d
    for k in range(4):
        if k > 0:

            @pl.when(y == k)
            def _(s=s, d=d):
                before_ref[0:128, :] = s
                before_ref[128:PACK, :] = d

        piece = held[lax.rem(k - y + 4, 4)]
        s = piece[128:129] * s + piece[0:128]
        d = piece[128:PACK] * d
    total_ref[0:128, :] = s
    total_ref[128:PACK, :] = d


def enter_kernel(z1_ref, z2_ref, z3_ref, yb_ref, out_ref):
    s = z3_ref[0:128, :]
    s = z2_ref[128:129, :] * s + z2_ref[0:128, :]
    s = z1_ref[128:129, :] * s + z1_ref[0:128, :]
    out_ref[...] = yb_ref[128:129, :] * s + yb_ref[0:128, :]


def finish_kernel(mech_ref, qs_ref, mine_ref, given_ref, other_ref, gate_ref, gain_ref, out_ref):
    given = given_ref[...]
    s = jnp.where(
        lax.axis_index(C) == 1, other_ref[128:129, :] * given + other_ref[0:128, :], mine_ref[...]
    )
    head = _first_head()
    s0 = jnp.where(head, s, 0.0).astype(bf16)
    s1 = jnp.where(head, 0.0, s).astype(bf16)
    gain = gain_ref[...]
    for n in range(TOK // 128):
        rows = slice(n * 128, (n + 1) * 128)
        for h, sh in enumerate((s0, s1)):
            cols = slice(h * DV, (h + 1) * DV)
            o = mech_ref[rows, cols] + _dot(qs_ref[rows, :], sh, NT)
            o = o * lax.rsqrt(jnp.mean(o * o, axis=-1, keepdims=True) + EPS) * gain
            out_ref[rows, cols] = (o * _silu(gate_ref[rows, cols].astype(f32))).astype(bf16)


OFFSETS = (0, 3, 1, 2)
SLOTS = tuple((j, i) for j in range(4) for i in range(4))


def chip_of(core, j, i):
    dz, dy = (i, j) if core == 0 else (j, i)
    z = lax.rem(lax.axis_index(Z) + OFFSETS[dz], 4)
    y = lax.rem(lax.axis_index(Y) + OFFSETS[dy], 4)
    return z * 4 + y


def chip_columns(chip):
    return pl.ds(pl.multiple_of(chip * 128, 128), 128)


def left_half():
    return lax.broadcasted_iota(jnp.int32, (1, 128), 1) < 64


def reorder(src_ref, dst_ref, rows):
    c = lax.axis_index(C)
    left = left_half()
    for core in range(2):
        base = jnp.where(c == core, 0, 1024)
        for t in range(8):
            one = src_ref[:, chip_columns(chip_of(core, *SLOTS[2 * t]))]
            two = src_ref[:, chip_columns(chip_of(core, *SLOTS[2 * t + 1]))]
            if core == 0:
                both = jnp.where(left, one, pltpu.roll(two, 64, 1))
            else:
                both = jnp.where(left, pltpu.roll(one, 64, 1), two)
            at = pl.ds(pl.multiple_of(base + t * 128, 128), 128)
            dst_ref[rows, at] = both.astype(bf16)


ROWS = TOK // 4


def place_rows(w_ref, got, sib):
    c = lax.axis_index(C)
    w_ref[pl.ds(pl.multiple_of(c * 128, 128), 128), :] = got[...]
    w_ref[pl.ds(pl.multiple_of((1 - c) * 128, 128), 128), :] = sib[...]


def attend_kernel(m0, m1, m2, own_w, got1, got2, sib1, sib2, x_ref, part_ref, w_ref):
    w_ref[0] = own_w[...]
    place_rows(w_ref.at[1], got1, sib1)
    place_rows(w_ref.at[2], got2, sib2)

    def block(n, _):
        rows = pl.ds(pl.multiple_of(n * ROWS, ROWS), ROWS)
        mixed = jnp.concatenate([m[rows, :] for m in (m0, m1, m2)], axis=1)
        part_ref[rows, :] = x_ref[rows, :].astype(f32) + _dot(mixed, w_ref[...].reshape(768, D))
        return 0

    lax.fori_loop(0, 4, block, 0)


def norm_kernel(
    part_ref, early, late, got3, sib3, gain_ref, normed_ref, tail_ref, resid_ref, w_ref, n_ref
):
    place_rows(w_ref, got3, sib3)
    gain = gain_ref[...]
    xi = lax.axis_index(X)

    def block(n, _):
        rows = pl.ds(pl.multiple_of(n * ROWS, ROWS), ROWS)
        within = pl.ds(pl.multiple_of(lax.rem(n, 2) * ROWS, ROWS), ROWS)
        mixed = jnp.where(n < 2, early[within, :], late[within, :])
        acc = part_ref[rows, :] + _dot(mixed, w_ref[...])

        @pl.when(xi == n)
        def _():
            resid_ref[...] = acc

        scaled = acc * lax.rsqrt(jnp.mean(acc * acc, axis=-1, keepdims=True) + EPS)
        n_ref[...] = scaled * gain

        @pl.when(n == 3)
        def _():
            tail_ref[...] = n_ref[ROWS - HALO :, :].astype(bf16)

        reorder(n_ref, normed_ref, rows)
        return 0

    lax.fori_loop(0, 4, block, 0)


SEG = HALO + ROWS
CHUNKS = tuple((a, min(256, HID - a)) for a in range(0, HID, 256))


def feed_kernel(rels, plan, x_ref, halo_ref, tg_ref, tv_ref, *refs):
    own, sib, refs = refs[:8], refs[8:16], refs[16:]
    out_refs, refs = refs[: len(plan)], refs[len(plan) :]
    xs_ref, hf_ref, hs_ref, g_ref, h_ref = refs
    hf_ref[...] = halo_ref[...].astype(f32)
    reorder(hf_ref, hs_ref, slice(None))
    xi = lax.axis_index(X)
    for s, rel in enumerate(rels):
        block = lax.rem(xi + rel, 4)
        at = pl.multiple_of(block * ROWS, ROWS)
        ahead = pl.multiple_of(jnp.maximum(at - HALO, 0), HALO)
        xs_ref[s * SEG : s * SEG + HALO, :] = jnp.where(
            block == 0, hs_ref[...], x_ref[pl.ds(ahead, HALO), :]
        )
        xs_ref[s * SEG + HALO : (s + 1) * SEG, :] = x_ref[pl.ds(at, ROWS), :]

    def blocks(arrays, part, cols):
        return [w[:, part, :, cols].reshape(w.shape[0] * 64, cols.stop - cols.start) for w in arrays]

    def project(n):
        a, wide = CHUNKS[n]
        for part in range(2):
            cols = slice(a, a + wide)
            w = jnp.concatenate(blocks(own, part, cols) + blocks(sib, part, cols), axis=0)
            new = _dot(xs_ref[...], w).astype(bf16).astype(f32)
            g_ref[n % 2, :, part * 256 : part * 256 + wide] = new

    def mix_columns(n):
        a, wide = CHUNKS[n]
        cols = slice(a, a + wide)
        for s in range(len(rels)):
            r = s * SEG + HALO
            mixes = []
            for part, t_ref in enumerate((tg_ref, tv_ref)):
                taps = t_ref[:, cols].astype(f32)
                at = slice(part * 256, part * 256 + wide)
                mix = taps[0:1] * g_ref[n % 2, r - 2 : r - 2 + ROWS, at]
                mix = mix + taps[1:2] * g_ref[n % 2, r - 1 : r - 1 + ROWS, at]
                mixes.append(mix + taps[2:3] * g_ref[n % 2, r : r + ROWS, at])
            h_ref[s * ROWS : (s + 1) * ROWS, cols] = (_silu(mixes[0]) * mixes[1]).astype(bf16)

    for n in range(len(CHUNKS)):
        project(n)
        if n > 0:
            mix_columns(n - 1)
    mix_columns(len(CHUNKS) - 1)
    for half, arrays in enumerate((own, sib)):
        rows = blocks(arrays, 2, slice(0, HID))
        for n, w in enumerate((rows[:4], rows[4:])):
            new = _dot(h_ref[...], jnp.concatenate(w, axis=0), NT)
            cols = slice(n * 512, n * 512 + 512)
            for (block, want), out_ref in zip(plan, out_refs):
                if want == half:
                    out_ref[:, cols] = new[block * ROWS : (block + 1) * ROWS].astype(out_ref.dtype)


def add_kernel(p_ref, ap_ref, m_ref, am_ref, out_p, out_m):
    out_p[...] = (p_ref[...] + ap_ref[...].astype(f32)).astype(bf16)
    out_m[...] = (m_ref[...] + am_ref[...].astype(f32)).astype(bf16)


def last_kernel(resid_ref, own_a, own_b, l_a, l_b, r_a, r_b, out_ref):
    first = lax.axis_index(C) == 0
    left = left_half()

    def total(g):
        cols = slice(g * 128, (g + 1) * 128)
        a = own_a[:, cols] + l_a[:, cols].astype(f32) + r_a[:, cols].astype(f32)
        b = own_b[:, cols] + l_b[:, cols].astype(f32) + r_b[:, cols].astype(f32)
        return jnp.where(first, a, b), jnp.where(first, b, a)

    totals = [total(g) for g in range(8)]
    for j, i in SLOTS:
        low, high = j * 4 + i, i * 4 + j
        one, two = totals[low // 2][0], totals[high // 2][1]
        one = one if low % 2 == 0 else pltpu.roll(one, 64, 1)
        two = two if high % 2 == 1 else pltpu.roll(two, 64, 1)
        cols = chip_columns(chip_of(0, j, i))
        out_ref[:, cols] = (resid_ref[:, cols] + jnp.where(left, one, two)).astype(bf16)


def by_first_core(step):
    pairs = []
    for z in range(4 - step):
        for y in range(4):
            pairs.append(((z * 4 + y) * 2, ((z + step) * 4 + y) * 2))
    return pairs


def ring(step):
    return [(i, (i + step) % 4) for i in range(4)]


def shape(*dims, dtype=bf16):
    return jax.ShapeDtypeStruct(dims, dtype)


def call(kernel, out_shape, n_in, cost, scratch=(), mib=8, n_hbm=0):
    out_specs = jax.tree.map(lambda _: VMEM, out_shape)
    return pl.pallas_call(
        kernel,
        out_shape=out_shape,
        in_specs=[VMEM] * n_in + [HBM] * n_hbm,
        out_specs=out_specs,
        scratch_shapes=list(scratch),
        compiler_params=_params(mib),
        cost_estimate=cost,
    )


HBM = pl.BlockSpec(memory_space=pltpu.HBM)
FEED_MIB = 20
ATTEND_MIB = 20


def feed(normed, halo, t_gate, t_value, pieces, rels, plan, dtypes):
    rows = SEG * len(rels)
    return pl.pallas_call(
        functools.partial(feed_kernel, rels, plan),
        out_shape=[shape(ROWS, 1024, dtype=d) for d in dtypes],
        in_specs=[VMEM] * 20,
        out_specs=[VMEM for _ in plan],
        scratch_shapes=[
            pltpu.VMEM((rows, D), bf16),
            pltpu.VMEM((HALO, D), f32),
            pltpu.VMEM((HALO, D), bf16),
            pltpu.VMEM((2, rows, 512), f32),
            pltpu.VMEM((ROWS * len(rels), HID), bf16),
        ],
        compiler_params=_params(FEED_MIB),
        cost_estimate=_cost(2 * rows * D * 3 * HID, 3 * D * HID * 2),
        name="feed",
    )(normed, halo, t_gate, t_value, *pieces)


def around(step, second):
    pairs = []
    for z in range(4):
        for y in range(4):
            for c in range(2):
                along_z = (c == 0) != second
                to = ((z + step) % 4, y, c) if along_z else (z, (y + step) % 4, c)
                pairs.append(((z * 4 + y) * 2 + c, (to[0] * 4 + to[1]) * 2 + c))
    return pairs


def per_device(
    x, q, k, v, switch, pre, fade, head_gain, w_out, ff_gain, w_gate, w_value, t_gate, t_value, w_down
):
    c = lax.axis_index(C)
    swap = [(0, 1), (1, 0)]

    steps = (1, 3, 2)
    shard = jnp.stack([w_gate, w_value, w_down.T], axis=0)
    first = [lax.ppermute(shard, SP, around(s, False)) for s in steps]

    cum, pack = call(
        state_kernel,
        (shape(TOK, 128, dtype=f32), shape(PACK, 128, dtype=f32)),
        0, _cost(2 * TOK * 128 * 256, 1e6),
        [
            pltpu.VMEM((TOK, 128), bf16), pltpu.VMEM((TOK, 128), bf16), pltpu.VMEM((6, 128), f32),
            pltpu.VMEM((TOK, 128), bf16), pltpu.VMEM((TOK, 256), bf16), pltpu.SemaphoreType.DMA((4,)),
        ], 8, 4,
    )(pre, fade.reshape(6, 128), k, v)
    other = lax.ppermute(pack, C, swap)

    w_half = lax.dynamic_slice_in_dim(w_out, c * 128, 128, 0)
    w_got = [lax.ppermute(w_half, X, ring(s)) for s in steps]

    chip = call(chip_kernel, shape(PACK, 128, dtype=f32), 2, _cost(1e5, 2e5))(pack, other)
    along_y = [lax.ppermute(chip, Y, ring(s)) for s in (3, 2, 1)]
    mech, q_shard = call(
        local_kernel, (shape(TOK, 256, dtype=f32), shape(TOK, 128)), 4,
        _cost(12 * 2 * 128 * 128 * 64 * 8, 3e6),
    )(q, k, v, cum)
    plane, before = call(
        plane_kernel, (shape(PACK, 128, dtype=f32), shape(PACK, 128, dtype=f32)), 4,
        _cost(1e5, 4e5), [pltpu.VMEM((4, PACK, 128), f32)],
    )(chip, *along_y)
    along_z = [lax.ppermute(plane, SP, by_first_core(s)) for s in (1, 2, 3)]
    entering = call(enter_kernel, shape(128, 128, dtype=f32), 4, _cost(1e5, 3e5))(*along_z, before)
    given = lax.ppermute(entering, C, [(0, 1)])
    stacks = [jnp.stack([shard, first[0]], axis=0), jnp.stack(first[1:], axis=0)]
    right, left = around(1, True), around(3, True)
    right_a = lax.ppermute(stacks[0], SP, right)
    left_b = lax.ppermute(stacks[1], SP, left)
    right_b = lax.ppermute(stacks[1], SP, right)
    left_a = lax.ppermute(stacks[0], SP, left)
    mixed = call(
        finish_kernel, shape(TOK, 256), 7, _cost(2 * TOK * 128 * 256, 3e6)
    )(mech, q_shard, entering, given, other, switch, head_gain.reshape(1, DV))

    from_left, from_right = lax.ppermute(mixed, X, ring(1)), lax.ppermute(mixed, X, ring(3))
    opposite = [
        lax.ppermute(from_left[: TOK // 2], X, ring(1)),
        lax.ppermute(from_right[TOK // 2 :], X, ring(3)),
    ]
    w_sib = [lax.ppermute(w, C, swap) for w in w_got]
    far = [lax.ppermute(right_a, SP, right), lax.ppermute(left_b, SP, left)]
    mine = [*stacks, right_a, right_b, left_a, left_b, *far]
    pieces = mine + [lax.ppermute(w, C, swap) for w in mine]
    (part,) = call(
        attend_kernel, [shape(TOK, D, dtype=f32)], 9,
        _cost(2 * TOK * 768 * D, 1.2e7), [pltpu.VMEM((3, 256, D), bf16)], ATTEND_MIB,
    )(mixed, from_left, from_right, w_out, *w_got[:2], *w_sib[:2], x)
    normed, tail, resid = call(
        norm_kernel,
        (shape(TOK, D), shape(HALO, D), shape(ROWS, D, dtype=f32)), 6,
        _cost(2 * TOK * 256 * D, 1.2e7),
        [pltpu.VMEM((256, D), bf16), pltpu.VMEM((ROWS, D), f32)], ATTEND_MIB,
    )(part, *opposite, w_got[2], w_sib[2], ff_gain.reshape(1, D))
    halo = lax.ppermute(tail, SP, [(i, i + 1) for i in range(31)])

    feeds = functools.partial(feed, normed, halo, t_gate, t_value, pieces)
    opp_a, opp_b = feeds((2,), ((0, 0), (0, 1)), (bf16, bf16))
    far_r = lax.ppermute(opp_a, X, ring(1))
    far_l = lax.ppermute(opp_b, X, ring(3))
    next_a, next_b, prev_a, prev_b = feeds(
        (1, 3), ((0, 0), (0, 1), (1, 0), (1, 1)), (f32, bf16, bf16, f32)
    )
    near_l_b = lax.ppermute(next_b, X, ring(1))
    near_r_a = lax.ppermute(prev_a, X, ring(3))
    send_r, send_l = call(
        add_kernel, (shape(ROWS, 1024), shape(ROWS, 1024)), 4, _cost(4e5, 4e6)
    )(next_a, far_r, prev_b, far_l)
    near_l_a = lax.ppermute(send_r, X, ring(1))
    near_r_b = lax.ppermute(send_l, X, ring(3))
    own_a, own_b = feeds((0,), ((0, 0), (0, 1)), (f32, f32))
    return call(last_kernel, shape(ROWS, D), 7, _cost(1e6, 5e6))(
        resid, own_a, own_b, near_l_a, near_l_b, near_r_a, near_r_b
    )


def solution(mesh):
    torus = Mesh(mesh.devices.reshape(4, 4, 2, 4), (Z, Y, C, X))
    return jax.shard_map(
        per_device,
        mesh=torus,
        in_specs=(
            P(SP, None), P(SP, X), P(SP, X), P(SP, X), P(SP, X), P(SP, X), P(SP), P(),
            P(X, None), P(), P(SP, X), P(SP, X), P(None, X), P(None, X), P(X, SP),
        ),
        out_specs=P((Z, Y, C, X), None),
        check_vma=False,
    )
```

```python
import functools
import jax
import jax.numpy as jnp
from jax import lax
from jax.experimental import pallas as pl
from jax.experimental.pallas import tpu as pltpu
from jax.sharding import Mesh
from jax.sharding import PartitionSpec as P


DK = 64
DV = 128
BLOCK = 64
TOK = 768
D = 2048
HID = 1408
HALO = 16
Z, Y, C, X = "z", "y", "c", "x"
SP = (Z, Y, C)
EPS = 1e-06
f32 = jnp.float32
bf16 = jnp.bfloat16
NT = (((1,), (1,)), ((), ()))
TN = (((0,), (0,)), ((), ()))
PACK = 136
VMEM = pl.BlockSpec(memory_space=pltpu.VMEM)


def _params(mib=40, sem=None):
    return pltpu.CompilerParams(vmem_limit_bytes=mib * 1024 * 1024, dimension_semantics=sem)


def _cost(flops, nbytes, trans=0):
    return pl.CostEstimate(flops=int(flops), bytes_accessed=int(nbytes), transcendentals=int(trans))


def _dot(a, b, dims=None):
    if dims is None:
        dims = (((1,), (0,)), ((), ()))
    return lax.dot_general(a, b, dims, preferred_element_type=f32)


def _log_sigmoid(x):
    return jnp.minimum(x, 0.0) - jnp.log1p(jnp.exp(-jnp.abs(x)))


def _silu(x):
    return x / (1.0 + jnp.exp(-x))


def _first_head():
    return lax.broadcasted_iota(jnp.int32, (1, 2 * DK), 1) < DK


def state_kernel(
    pre_hbm, fade_hbm, k_hbm, v_hbm, cum_ref, pack_ref, kf_ref, pre_ref, fade_ref, k_ref, v_ref, sems
):
    pairs = ((pre_hbm, pre_ref), (fade_hbm, fade_ref), (k_hbm, k_ref), (v_hbm, v_ref))
    copies = [pltpu.make_async_copy(*pair, sems.at[n]) for n, pair in enumerate(pairs)]
    for copy in copies:
        copy.start()
    for copy in copies:
        copy.wait()
    row = lax.broadcasted_iota(jnp.int32, (128, 128), 0)
    col = lax.broadcasted_iota(jnp.int32, (128, 128), 1)
    lower = ((row >= col) & ((row < BLOCK) == (col < BLOCK))).astype(f32)
    ones = jnp.ones((128, 128), f32)
    high = lax.Precision.HIGHEST
    cums = []
    for n in range(TOK // 128):
        rows = slice(n * 128, (n + 1) * 128)
        rate = _log_sigmoid(pre_ref[rows, :].astype(f32)) * (1.0 / 16.0)
        cum = jnp.dot(lower, rate, precision=high, preferred_element_type=f32)
        cum = cum + jnp.dot(
            lower * fade_ref[n : n + 1, :], ones, precision=high, preferred_element_type=f32
        )
        cum_ref[rows, :] = cum
        cums.append(cum)
    suffix = jnp.zeros((1, 2 * DK), f32)
    for b in reversed(range(TOK // BLOCK)):
        n, half = divmod(b, 2)
        cum = cums[n][half * BLOCK : (half + 1) * BLOCK]
        total = cum[BLOCK - 1 : BLOCK]
        rows = slice(b * BLOCK, (b + 1) * BLOCK)
        kf_ref[rows, :] = (k_ref[rows, :].astype(f32) * jnp.exp(suffix + total - cum)).astype(bf16)
        suffix = suffix + total
    kf = kf_ref[...]
    first = _dot(v_ref[:, :DV], kf, TN)
    second = _dot(v_ref[:, DV:], kf, TN)
    pack_ref[0:128, :] = jnp.where(_first_head(), first, second)
    pack_ref[128:PACK, :] = jnp.broadcast_to(jnp.exp(suffix), (8, 128))


def local_kernel(q_ref, k_ref, v_ref, cum_ref, mech_ref, qs_ref):
    head = _first_head()
    row = lax.broadcasted_iota(jnp.int32, (128, BLOCK), 0)
    col = lax.broadcasted_iota(jnp.int32, (128, BLOCK), 1)
    lower = jnp.where(row < BLOCK, row, row - BLOCK) >= col
    state = jnp.zeros((DV, 2 * DK), f32)
    before = jnp.zeros((1, 2 * DK), f32)
    for b in range(TOK // BLOCK):
        rows = slice(b * BLOCK, (b + 1) * BLOCK)
        cum = cum_ref[rows, :]
        total = cum[BLOCK - 1 : BLOCK]
        q = q_ref[rows, :].astype(f32) * DK**-0.5
        k = k_ref[rows, :].astype(f32)
        qd = q * jnp.exp(cum)
        qs_ref[rows, :] = (q * jnp.exp(cum + before)).astype(bf16)
        both = jnp.concatenate([jnp.where(head, qd, 0.0), jnp.where(head, 0.0, qd)], 0).astype(bf16)
        grown = (k * jnp.exp(-cum)).astype(bf16)
        faded = (k * jnp.exp(total - cum)).astype(bf16)
        scores = _dot(both, grown, NT)
        scores = jnp.where(lower, scores, 0.0).astype(bf16)
        inter = _dot(both, state.astype(bf16), NT)
        v0, v1 = v_ref[rows, :DV], v_ref[rows, DV:]
        mech_ref[rows, :DV] = _dot(scores[:BLOCK], v0) + inter[:BLOCK]
        mech_ref[rows, DV:] = _dot(scores[BLOCK:], v1) + inter[BLOCK:]
        update = jnp.where(head, _dot(v0, faded, TN), _dot(v1, faded, TN))
        state = state * jnp.exp(total) + update
        before = before + total


def chip_kernel(own_ref, other_ref, chip_ref):
    second = lax.axis_index(C) == 1
    own_s, own_d = own_ref[0:128, :], own_ref[128:PACK, :]
    oth_s, oth_d = other_ref[0:128, :], other_ref[128:PACK, :]
    s = jnp.where(second, own_d[0:1] * oth_s + own_s, oth_d[0:1] * own_s + oth_s)
    chip_ref[0:128, :] = s
    chip_ref[128:PACK, :] = own_d * oth_d


def plane_kernel(own_ref, up_ref, opp_ref, down_ref, total_ref, before_ref, held):
    y = lax.axis_index(Y)
    held[0] = own_ref[...]
    held[1] = up_ref[...]
    held[2] = opp_ref[...]
    held[3] = down_ref[...]
    s = jnp.zeros((128, 128), f32)
    d = jnp.ones((8, 128), f32)
    before_ref[0:128, :] = s
    before_ref[128:PACK, :] = d
    for k in range(4):
        if k > 0:

            @pl.when(y == k)
            def _(s=s, d=d):
                before_ref[0:128, :] = s
                before_ref[128:PACK, :] = d

        piece = held[lax.rem(k - y + 4, 4)]
        s = piece[128:129] * s + piece[0:128]
        d = piece[128:PACK] * d
    total_ref[0:128, :] = s
    total_ref[128:PACK, :] = d


def enter_kernel(z1_ref, z2_ref, z3_ref, yb_ref, out_ref):
    s = z3_ref[0:128, :]
    s = z2_ref[128:129, :] * s + z2_ref[0:128, :]
    s = z1_ref[128:129, :] * s + z1_ref[0:128, :]
    out_ref[...] = yb_ref[128:129, :] * s + yb_ref[0:128, :]


def finish_kernel(mech_ref, qs_ref, mine_ref, given_ref, other_ref, gate_ref, gain_ref, out_ref):
    given = given_ref[...]
    s = jnp.where(
        lax.axis_index(C) == 1, other_ref[128:129, :] * given + other_ref[0:128, :], mine_ref[...]
    )
    head = _first_head()
    s0 = jnp.where(head, s, 0.0).astype(bf16)
    s1 = jnp.where(head, 0.0, s).astype(bf16)
    gain = gain_ref[...]
    for n in range(TOK // 128):
        rows = slice(n * 128, (n + 1) * 128)
        for h, sh in enumerate((s0, s1)):
            cols = slice(h * DV, (h + 1) * DV)
            o = mech_ref[rows, cols] + _dot(qs_ref[rows, :], sh, NT)
            o = o * lax.rsqrt(jnp.mean(o * o, axis=-1, keepdims=True) + EPS) * gain
            out_ref[rows, cols] = (o * _silu(gate_ref[rows, cols].astype(f32))).astype(bf16)


OFFSETS = (0, 3, 1, 2)
SLOTS = tuple((j, i) for j in range(4) for i in range(4))


def chip_of(core, j, i):
    dz, dy = (i, j) if core == 0 else (j, i)
    z = lax.rem(lax.axis_index(Z) + OFFSETS[dz], 4)
    y = lax.rem(lax.axis_index(Y) + OFFSETS[dy], 4)
    return z * 4 + y


def chip_columns(chip):
    return pl.ds(pl.multiple_of(chip * 128, 128), 128)


def left_half():
    return lax.broadcasted_iota(jnp.int32, (1, 128), 1) < 64


def reorder(src_ref, dst_ref, rows):
    c = lax.axis_index(C)
    left = left_half()
    for core in range(2):
        base = jnp.where(c == core, 0, 1024)
        for t in range(8):
            one = src_ref[:, chip_columns(chip_of(core, *SLOTS[2 * t]))]
            two = src_ref[:, chip_columns(chip_of(core, *SLOTS[2 * t + 1]))]
            if core == 0:
                both = jnp.where(left, one, pltpu.roll(two, 64, 1))
            else:
                both = jnp.where(left, pltpu.roll(one, 64, 1), two)
            at = pl.ds(pl.multiple_of(base + t * 128, 128), 128)
            dst_ref[rows, at] = both.astype(bf16)


ROWS = TOK // 4


def place_rows(w_ref, got, sib):
    c = lax.axis_index(C)
    w_ref[pl.ds(pl.multiple_of(c * 128, 128), 128), :] = got[...]
    w_ref[pl.ds(pl.multiple_of((1 - c) * 128, 128), 128), :] = sib[...]


def attend_kernel(m0, m1, m2, own_w, got1, got2, sib1, sib2, x_ref, part_ref, w_ref):
    w_ref[0] = own_w[...]
    place_rows(w_ref.at[1], got1, sib1)
    place_rows(w_ref.at[2], got2, sib2)

    def block(n, _):
        rows = pl.ds(pl.multiple_of(n * ROWS, ROWS), ROWS)
        mixed = jnp.concatenate([m[rows, :] for m in (m0, m1, m2)], axis=1)
        part_ref[rows, :] = x_ref[rows, :].astype(f32) + _dot(mixed, w_ref[...].reshape(768, D))
        return 0

    lax.fori_loop(0, 4, block, 0)


def norm_kernel(
    part_ref, early, late, got3, sib3, gain_ref, normed_ref, tail_ref, resid_ref, w_ref, n_ref
):
    place_rows(w_ref, got3, sib3)
    gain = gain_ref[...]
    xi = lax.axis_index(X)

    def block(n, _):
        rows = pl.ds(pl.multiple_of(n * ROWS, ROWS), ROWS)
        within = pl.ds(pl.multiple_of(lax.rem(n, 2) * ROWS, ROWS), ROWS)
        mixed = jnp.where(n < 2, early[within, :], late[within, :])
        acc = part_ref[rows, :] + _dot(mixed, w_ref[...])

        @pl.when(xi == n)
        def _():
            resid_ref[...] = acc

        scaled = acc * lax.rsqrt(jnp.mean(acc * acc, axis=-1, keepdims=True) + EPS)
        n_ref[...] = scaled * gain

        @pl.when(n == 3)
        def _():
            tail_ref[...] = n_ref[ROWS - HALO :, :].astype(bf16)

        reorder(n_ref, normed_ref, rows)
        return 0

    lax.fori_loop(0, 4, block, 0)


def stack_kernel(own_ref, one_ref, two_ref, three_ref, near_ref, far_ref):
    near_ref[0] = own_ref[...]
    near_ref[1] = one_ref[...]
    far_ref[0] = two_ref[...]
    far_ref[1] = three_ref[...]


SEG = HALO + ROWS
CHUNKS = tuple((a, min(256, HID - a)) for a in range(0, HID, 256))


def feed_kernel(rels, plan, x_ref, halo_ref, tg_ref, tv_ref, *refs):
    own, sib, refs = refs[:8], refs[8:16], refs[16:]
    out_refs, refs = refs[: len(plan)], refs[len(plan) :]
    xs_ref, hf_ref, hs_ref, g_ref, h_ref = refs
    hf_ref[...] = halo_ref[...].astype(f32)
    reorder(hf_ref, hs_ref, slice(None))
    xi = lax.axis_index(X)
    for s, rel in enumerate(rels):
        block = lax.rem(xi + rel, 4)
        at = pl.multiple_of(block * ROWS, ROWS)
        ahead = pl.multiple_of(jnp.maximum(at - HALO, 0), HALO)
        xs_ref[s * SEG : s * SEG + HALO, :] = jnp.where(
            block == 0, hs_ref[...], x_ref[pl.ds(ahead, HALO), :]
        )
        xs_ref[s * SEG + HALO : (s + 1) * SEG, :] = x_ref[pl.ds(at, ROWS), :]

    def blocks(arrays, part, cols):
        return [w[:, part, :, cols].reshape(w.shape[0] * 64, cols.stop - cols.start) for w in arrays]

    def project(n):
        a, wide = CHUNKS[n]
        for part in range(2):
            cols = slice(a, a + wide)
            w = jnp.concatenate(blocks(own, part, cols) + blocks(sib, part, cols), axis=0)
            new = _dot(xs_ref[...], w).astype(bf16).astype(f32)
            g_ref[n % 2, :, part * 256 : part * 256 + wide] = new

    def mix_columns(n):
        a, wide = CHUNKS[n]
        cols = slice(a, a + wide)
        for s in range(len(rels)):
            r = s * SEG + HALO
            mixes = []
            for part, t_ref in enumerate((tg_ref, tv_ref)):
                taps = t_ref[:, cols].astype(f32)
                at = slice(part * 256, part * 256 + wide)
                mix = taps[0:1] * g_ref[n % 2, r - 2 : r - 2 + ROWS, at]
                mix = mix + taps[1:2] * g_ref[n % 2, r - 1 : r - 1 + ROWS, at]
                mixes.append(mix + taps[2:3] * g_ref[n % 2, r : r + ROWS, at])
            h_ref[s * ROWS : (s + 1) * ROWS, cols] = (_silu(mixes[0]) * mixes[1]).astype(bf16)

    for n in range(len(CHUNKS)):
        project(n)
        if n > 0:
            mix_columns(n - 1)
    mix_columns(len(CHUNKS) - 1)
    for half, arrays in enumerate((own, sib)):
        rows = blocks(arrays, 2, slice(0, HID))
        for n, w in enumerate((rows[:4], rows[4:])):
            new = _dot(h_ref[...], jnp.concatenate(w, axis=0), NT)
            cols = slice(n * 512, n * 512 + 512)
            for (block, want), out_ref in zip(plan, out_refs):
                if want == half:
                    out_ref[:, cols] = new[block * ROWS : (block + 1) * ROWS].astype(out_ref.dtype)


def add_kernel(p_ref, ap_ref, m_ref, am_ref, out_p, out_m):
    out_p[...] = (p_ref[...] + ap_ref[...].astype(f32)).astype(bf16)
    out_m[...] = (m_ref[...] + am_ref[...].astype(f32)).astype(bf16)


def add_in_order(base_ref, parts_a, parts_b, out_ref):
    first = lax.axis_index(C) == 0
    left = left_half()

    def total(g):
        cols = slice(g * 128, (g + 1) * 128)
        a = sum(ref[:, cols].astype(f32) for ref in parts_a)
        b = sum(ref[:, cols].astype(f32) for ref in parts_b)
        return jnp.where(first, a, b), jnp.where(first, b, a)

    totals = [total(g) for g in range(8)]
    for j, i in SLOTS:
        low, high = j * 4 + i, i * 4 + j
        one, two = totals[low // 2][0], totals[high // 2][1]
        one = one if low % 2 == 0 else pltpu.roll(one, 64, 1)
        two = two if high % 2 == 1 else pltpu.roll(two, 64, 1)
        cols = chip_columns(chip_of(0, j, i))
        out_ref[:, cols] = (base_ref[:, cols] + jnp.where(left, one, two)).astype(out_ref.dtype)


def base_kernel(resid_ref, own_a, own_b, r_a, l_b, out_ref):
    add_in_order(resid_ref, (own_a, r_a), (own_b, l_b), out_ref)


def last_kernel(base_ref, l_a, r_b, out_ref):
    add_in_order(base_ref, (l_a,), (r_b,), out_ref)


def by_first_core(step):
    pairs = []
    for z in range(4 - step):
        for y in range(4):
            pairs.append(((z * 4 + y) * 2, ((z + step) * 4 + y) * 2))
    return pairs


def ring(step):
    return [(i, (i + step) % 4) for i in range(4)]


def shape(*dims, dtype=bf16):
    return jax.ShapeDtypeStruct(dims, dtype)


def call(kernel, out_shape, n_in, cost, scratch=(), mib=5, n_hbm=0):
    out_specs = jax.tree.map(lambda _: VMEM, out_shape)
    return pl.pallas_call(
        kernel,
        out_shape=out_shape,
        in_specs=[VMEM] * n_in + [HBM] * n_hbm,
        out_specs=out_specs,
        scratch_shapes=list(scratch),
        compiler_params=_params(mib),
        cost_estimate=cost,
    )


HBM = pl.BlockSpec(memory_space=pltpu.HBM)
FEED_MIB = 12
ATTEND_MIB = 10


def feed(normed, halo, t_gate, t_value, pieces, rels, plan, dtypes):
    rows = SEG * len(rels)
    return pl.pallas_call(
        functools.partial(feed_kernel, rels, plan),
        out_shape=[shape(ROWS, 1024, dtype=d) for d in dtypes],
        in_specs=[VMEM] * 20,
        out_specs=[VMEM for _ in plan],
        scratch_shapes=[
            pltpu.VMEM((rows, D), bf16),
            pltpu.VMEM((HALO, D), f32),
            pltpu.VMEM((HALO, D), bf16),
            pltpu.VMEM((2, rows, 512), f32),
            pltpu.VMEM((ROWS * len(rels), HID), bf16),
        ],
        compiler_params=_params(FEED_MIB),
        cost_estimate=_cost(2 * rows * D * 3 * HID, 3 * D * HID * 2),
        name="feed",
    )(normed, halo, t_gate, t_value, *pieces)


def around(step, second):
    pairs = []
    for z in range(4):
        for y in range(4):
            for c in range(2):
                along_z = (c == 0) != second
                to = ((z + step) % 4, y, c) if along_z else (z, (y + step) % 4, c)
                pairs.append(((z * 4 + y) * 2 + c, (to[0] * 4 + to[1]) * 2 + c))
    return pairs


def per_device(
    x, q, k, v, switch, pre, fade, head_gain, w_out, ff_gain, w_gate, w_value, t_gate, t_value, w_down
):
    c = lax.axis_index(C)
    swap = [(0, 1), (1, 0)]

    steps = (1, 3, 2)
    shard = jnp.stack([w_gate, w_value, w_down.T], axis=0)
    first = [lax.ppermute(shard, SP, around(s, False)) for s in steps]

    cum, pack = call(
        state_kernel,
        (shape(TOK, 128, dtype=f32), shape(PACK, 128, dtype=f32)),
        0, _cost(2 * TOK * 128 * 256, 1e6),
        [
            pltpu.VMEM((TOK, 128), bf16), pltpu.VMEM((TOK, 128), bf16), pltpu.VMEM((6, 128), f32),
            pltpu.VMEM((TOK, 128), bf16), pltpu.VMEM((TOK, 256), bf16), pltpu.SemaphoreType.DMA((4,)),
        ], 5, 4,
    )(pre, fade.reshape(6, 128), k, v)
    other = lax.ppermute(pack, C, swap)

    w_half = lax.dynamic_slice_in_dim(w_out, c * 128, 128, 0)
    w_got = [lax.ppermute(w_half, X, ring(s)) for s in steps]

    chip = call(chip_kernel, shape(PACK, 128, dtype=f32), 2, _cost(1e5, 2e5))(pack, other)
    along_y = [lax.ppermute(chip, Y, ring(s)) for s in (3, 2, 1)]
    mech, q_shard = call(
        local_kernel, (shape(TOK, 256, dtype=f32), shape(TOK, 128)), 4,
        _cost(12 * 2 * 128 * 128 * 64 * 8, 3e6),
    )(q, k, v, cum)
    plane, before = call(
        plane_kernel, (shape(PACK, 128, dtype=f32), shape(PACK, 128, dtype=f32)), 4,
        _cost(1e5, 4e5), [pltpu.VMEM((4, PACK, 128), f32)],
    )(chip, *along_y)
    along_z = [lax.ppermute(plane, SP, by_first_core(s)) for s in (1, 2, 3)]
    entering = call(enter_kernel, shape(128, 128, dtype=f32), 4, _cost(1e5, 3e5))(*along_z, before)
    given = lax.ppermute(entering, C, [(0, 1)])
    stacks = call(
        stack_kernel, [shape(2, 3, 64, HID)] * 2, 4, _cost(1e5, 4 * 3 * 64 * HID * 4)
    )(shard, *first)
    right, left = around(1, True), around(3, True)
    right_a = lax.ppermute(stacks[0], SP, right)
    left_b = lax.ppermute(stacks[1], SP, left)
    right_b = lax.ppermute(stacks[1], SP, right)
    left_a = lax.ppermute(stacks[0], SP, left)
    mixed = call(
        finish_kernel, shape(TOK, 256), 7, _cost(2 * TOK * 128 * 256, 3e6)
    )(mech, q_shard, entering, given, other, switch, head_gain.reshape(1, DV))

    from_left, from_right = lax.ppermute(mixed, X, ring(1)), lax.ppermute(mixed, X, ring(3))
    opposite = [
        lax.ppermute(from_left[: TOK // 2], X, ring(1)),
        lax.ppermute(from_right[TOK // 2 :], X, ring(3)),
    ]
    w_sib = [lax.ppermute(w, C, swap) for w in w_got]
    far = [lax.ppermute(right_a, SP, right), lax.ppermute(left_b, SP, left)]
    mine = [*stacks, right_a, right_b, left_a, left_b, *far]
    pieces = mine + [lax.ppermute(w, C, swap) for w in mine]
    (part,) = call(
        attend_kernel, [shape(TOK, D, dtype=f32)], 9,
        _cost(2 * TOK * 768 * D, 1.2e7), [pltpu.VMEM((3, 256, D), bf16)], ATTEND_MIB,
    )(mixed, from_left, from_right, w_out, *w_got[:2], *w_sib[:2], x)
    normed, tail, resid = call(
        norm_kernel,
        (shape(TOK, D), shape(HALO, D), shape(ROWS, D, dtype=f32)), 6,
        _cost(2 * TOK * 256 * D, 1.2e7),
        [pltpu.VMEM((256, D), bf16), pltpu.VMEM((ROWS, D), f32)], ATTEND_MIB,
    )(part, *opposite, w_got[2], w_sib[2], ff_gain.reshape(1, D))
    halo = lax.ppermute(tail, SP, [(i, i + 1) for i in range(31)])

    feeds = functools.partial(feed, normed, halo, t_gate, t_value, pieces)
    opp_a, opp_b = feeds((2,), ((0, 0), (0, 1)), (bf16, bf16))
    far_r = lax.ppermute(opp_a, X, ring(1))
    far_l = lax.ppermute(opp_b, X, ring(3))
    next_a, next_b, prev_a, prev_b = feeds(
        (1, 3), ((0, 0), (0, 1), (1, 0), (1, 1)), (f32, bf16, bf16, f32)
    )
    near_l_b = lax.ppermute(next_b, X, ring(1))
    near_r_a = lax.ppermute(prev_a, X, ring(3))
    send_r, send_l = call(
        add_kernel, (shape(ROWS, 1024), shape(ROWS, 1024)), 4, _cost(4e5, 4e6)
    )(next_a, far_r, prev_b, far_l)
    near_l_a = lax.ppermute(send_r, X, ring(1))
    near_r_b = lax.ppermute(send_l, X, ring(3))
    own_a, own_b = feeds((0,), ((0, 0), (0, 1)), (f32, f32))
    base = call(base_kernel, shape(ROWS, D, dtype=f32), 5, _cost(1e6, 6e6))(
        resid, own_a, own_b, near_r_a, near_l_b
    )
    return call(last_kernel, shape(ROWS, D), 3, _cost(1e6, 3e6))(base, near_l_a, near_r_b)


def solution(mesh):
    torus = Mesh(mesh.devices.reshape(4, 4, 2, 4), (Z, Y, C, X))
    return jax.shard_map(
        per_device,
        mesh=torus,
        in_specs=(
            P(SP, None), P(SP, X), P(SP, X), P(SP, X), P(SP, X), P(SP, X), P(SP), P(),
            P(X, None), P(), P(SP, X), P(SP, X), P(None, X), P(None, X), P(X, SP),
        ),
        out_specs=P((Z, Y, C, X), None),
        check_vma=False,
    )
```
